256 devices in a mesh: ep: 128 (over z, y, x), tp: 2 (over core).
Axes of the slice: x: 4, y: 4, z: 8, core: 2. Of those that a mesh axis runs over, the one named last changes fastest.
Arguments:
- tokens: bfloat16 [2048, 2048], P('ep'), may hold values from -6 to 6
- lengths: int32 [2048], P('ep'), may hold values from 1024 to 8191
- prior_state: float32 [2048, 16, 64, 64], P('ep', 'tp'), may hold values from -2 to 2
- mix_gain: float32 [2048], replicated, may hold values from 0.1 to 1.9
- post_gain: float32 [2048], replicated, may hold values from 0.1 to 1.9
- ffn_gain: float32 [2048], replicated, may hold values from 0.1 to 1.9
- out_gain: float32 [2048], replicated, may hold values from 0.1 to 1.9
- query_weight: bfloat16 [2048, 1024], P('ep', 'tp'), may hold values from -0.125 to 0.125
- key_weight: bfloat16 [2048, 1024], P('ep', 'tp'), may hold values from -0.125 to 0.125
- value_weight: bfloat16 [2048, 1024], P('ep', 'tp'), may hold values from -0.125 to 0.125
- gate_weight: bfloat16 [2048, 1024], P('ep', 'tp'), may hold values from -0.125 to 0.125
- out_weight: bfloat16 [1024, 2048], P('tp', 'ep'), may hold values from -0.1875 to 0.1875
- routes: int32 [2048, 6], P('ep'), may hold values from 0 to 127, all different within a row; in each aligned block of 16 rows (0 to 15, 16 to 31, ...) at most 2 rows name the same one
- route_gates: float32 [2048, 6], P('ep'), may hold values from 0.1 to 0.9
- expert_gate: bfloat16 [128, 2048, 512], P('ep', None, 'tp'), may hold values from -0.125 to 0.125
- expert_up: bfloat16 [128, 2048, 512], P('ep', None, 'tp'), may hold values from -0.125 to 0.125
- expert_down: bfloat16 [128, 512, 2048], P('ep', 'tp'), may hold values from -0.25 to 0.25
- shared_gate: bfloat16 [2048, 512], P(None, 'tp'), may hold values from -0.125 to 0.125
- shared_up: bfloat16 [2048, 512], P(None, 'tp'), may hold values from -0.125 to 0.125
- shared_down: bfloat16 [512, 2048], P('tp'), may hold values from -0.25 to 0.25
Outputs:
- result: bfloat16 [2048, 2048], P('ep')
- new_state: float32 [2048, 16, 64, 64], P('ep', 'tp')
The draws below stay inside these ranges and needn't reach their ends.
Inputs may be any that keep to these rules, and one draw needn't show every extreme that they name: `routes`: each row names 6 different experts. In the rows of one device (aligned blocks of 16 rows) no expert is named more than 2 times, and in every draw some expert is named exactly 2 times in some block.
All inputs are finite; a program needn't handle non-finite values.
Results may differ from the reference program's by a relative error of at most 0.02.
Values may be sent and summed in bfloat16 or wider, within the bound.
A program may use at most 128 MiB of HBM per device.

```python
import math
import jax
import jax.numpy as jnp
import numpy as np
from jax import lax

D = 2048
HEAD = 64
HEADS = 16
RW = 1024
FE = 512
FS = 512
TOPK = 6
SEQ_DEV = 16
TOKENS = 2048
EXPERTS = 128
CAP = 2
N_EP = 128
N_TP = 2


def with_ends(values, rng, least, top_value):
    place = [jax.random.randint(jax.random.fold_in(rng, axis), (), 0, length) for axis, length in enumerate(values.shape)]
    longest = values.shape.index(max(values.shape))
    beside = place[:longest] + [(place[longest] + 1) % values.shape[longest]] + place[longest + 1:]
    return values.at[tuple(place)].set(least).at[tuple(beside)].set(top_value)


def block_levels(key, extent, pieces, least, top_value):
    loudness = 1.0
    for position, shards_of in pieces:
        draws = jax.random.uniform(jax.random.fold_in(jax.random.fold_in(key, 6), position), (shards_of,), jnp.float32, least / len(pieces), top_value / len(pieces))
        loudness = loudness * jnp.repeat(jnp.exp(draws), extent[position] // shards_of).reshape((-1,) + (1,) * (len(extent) - 1 - position))
    return loudness


def assign_block(rng, own, number, rows, amount, top, reach, lean):
    sequence = jax.random.permutation(rng, amount)
    crowded, common = portions_of(amount, rows * top, reach, lean, True), portions_of(amount, rows * top, reach, lean, False)
    places = jnp.arange(amount)

    def named(sizes, offset_by):
        used = int((sizes > 0).sum())
        fixed = max(1, used // 4)
        passed = fixed + (places - fixed + offset_by * (used - fixed)) % max(1, amount - fixed)
        return jnp.zeros((amount,), jnp.int32).at[sequence[jnp.where(places < fixed, places, passed)]].set(jnp.asarray(sizes, jnp.int32))

    sizes = jnp.where(number % 4 == 0, named(crowded, number // 4), named(common, number - number // 4 - 1))
    mixed = jax.random.permutation(jax.random.fold_in(own, 3), amount)
    source_of, receiver = mixed[0:amount // 2 * 2:2], mixed[1:amount // 2 * 2:2]
    room = jnp.minimum(sizes[source_of] - 1, reach - sizes[receiver]) // 2
    room = jnp.where((source_of == sequence[0]) | (receiver == sequence[0]) | (sizes[receiver] == 0), 0, jnp.maximum(room, 0))
    passed = jax.random.randint(jax.random.fold_in(own, 4), (amount // 2,), 0, 1 << 20) % (room + 1)
    sizes = sizes.at[source_of].add(-passed).at[receiver].add(passed)
    members = jnp.searchsorted(jnp.cumsum(sizes), jnp.arange(rows * top), side="right").astype(jnp.int32)
    table = members.reshape(top, rows).T
    table = table[jax.random.permutation(jax.random.fold_in(own, 1), rows)]
    offset_by = jax.random.randint(jax.random.fold_in(own, 2), (rows, 1), 0, top)
    return jnp.take_along_axis(table, (jnp.arange(top)[None, :] + offset_by) % top, axis=1)


def portions_of(number_of, total, most, lean, full):
    weights = [(1 << 20) // math.isqrt(rank ** lean) + 1 for rank in range(1, number_of + 1)]
    largest = most if full else min(most, max(-(-total // number_of), total * weights[0] // sum(weights)))
    least = 1 if total - largest >= number_of - 1 else 0
    counts, rest = [largest] + [least] * (number_of - 1), total - largest - least * (number_of - 1)
    while rest > 0:
        movable = [i for i in range(1, number_of) if counts[i] < largest] or [i for i in range(1, number_of) if counts[i] < most]
        pool, budget = sum([weights[i] for i in movable]), rest
        for i in movable:
            extra = min(most - counts[i], max(1, budget * weights[i] // pool), rest)
            counts[i] = counts[i] + extra
            rest = rest - extra
    return np.array(counts)


def bell_draw(key, dims, spread, most, cuts=(), kind=jnp.bfloat16):
    array = spread * jax.random.normal(key, dims, jnp.float32)
    if cuts:
        array = array * block_levels(key, dims, cuts, -0.22, 0.18)
    return jnp.clip(array, -most, most).astype(kind)


def setup_inputs(seed: int = 0) -> dict:
    keys = jax.random.split(jax.random.key(seed), 21)
    tokens = bell_draw(keys[0], (TOKENS, D), 1.0, 6.0, ((0, 128),))
    lengths = with_ends(jax.random.randint(keys[1], (TOKENS,), 1024, 8192), jax.random.fold_in(keys[1], 1), 1024, 8191).astype(jnp.int32)
    prior_state = bell_draw(keys[2], (TOKENS, HEADS, HEAD, HEAD), 0.15, 2.0, ((0, 128), (1, 2)), jnp.float32)
    mix_gain = jnp.clip(1.0 + 0.18 * jax.random.normal(keys[3], (D,), jnp.float32), 0.1, 1.9)
    post_gain = jnp.clip(1.0 + 0.18 * jax.random.normal(keys[4], (D,), jnp.float32), 0.1, 1.9)
    ffn_gain = jnp.clip(1.0 + 0.18 * jax.random.normal(keys[5], (D,), jnp.float32), 0.1, 1.9)
    out_gain = jnp.clip(1.0 + 0.18 * jax.random.normal(keys[6], (D,), jnp.float32), 0.1, 1.9)
    query_weight = bell_draw(keys[7], (D, RW), D ** -0.5, 0.125, ((0, 128), (1, 2)))
    key_weight = bell_draw(keys[8], (D, RW), D ** -0.5, 0.125, ((0, 128), (1, 2)))
    value_weight = bell_draw(keys[9], (D, RW), D ** -0.5, 0.125, ((0, 128), (1, 2)))
    gate_weight = bell_draw(keys[10], (D, RW), D ** -0.5, 0.125, ((0, 128), (1, 2)))
    out_weight = bell_draw(keys[11], (RW, D), RW ** -0.5, 0.1875, ((0, 2), (1, 128)))
    routes_keys = jax.random.split(jax.random.fold_in(keys[12], 1), TOKENS // SEQ_DEV)
    routes_turns = jax.random.permutation(jax.random.fold_in(keys[12], 3), TOKENS // SEQ_DEV)
    routes = jax.vmap(lambda own, number: assign_block(jax.random.fold_in(keys[12], 2), own, number, SEQ_DEV, EXPERTS, TOPK, CAP, 2))(routes_keys, routes_turns).reshape((TOKENS, TOPK))
    route_gates = jnp.clip(0.1 + 0.79999997 * jax.random.uniform(keys[13], (TOKENS, TOPK), jnp.float32) ** block_levels(keys[13], (TOKENS, TOPK), ((0, 128),), -0.2, 0.2), 0.1, 0.9)
    expert_gate = bell_draw(keys[14], (EXPERTS, D, FE), D ** -0.5, 0.125, ((0, 128), (2, 2)))
    expert_up = bell_draw(keys[15], (EXPERTS, D, FE), D ** -0.5, 0.125, ((0, 128), (2, 2)))
    expert_down = bell_draw(keys[16], (EXPERTS, FE, D), FE ** -0.5, 0.25, ((0, 128), (1, 2)))
    shared_gate = bell_draw(keys[17], (D, FS), D ** -0.5, 0.125, ((1, 2),))
    shared_up = bell_draw(keys[18], (D, FS), D ** -0.5, 0.125, ((1, 2),))
    shared_down = bell_draw(keys[19], (FS, D), FS ** -0.5, 0.25, ((0, 2),))
    return {"tokens": tokens, "lengths": lengths, "prior_state": prior_state, "mix_gain": mix_gain, "post_gain": post_gain, "ffn_gain": ffn_gain, "out_gain": out_gain, "query_weight": query_weight, "key_weight": key_weight, "value_weight": value_weight, "gate_weight": gate_weight, "out_weight": out_weight, "routes": routes, "route_gates": route_gates, "expert_gate": expert_gate, "expert_up": expert_up, "expert_down": expert_down, "shared_gate": shared_gate, "shared_up": shared_up, "shared_down": shared_down}


EPS = 1e-06
THETA = 10000.0

def rounded(values):
    return lax.optimization_barrier(values.astype(jnp.bfloat16)).astype(jnp.float32)

def scaled_rows(values, gain_row):
    widened = values.astype(jnp.float32)
    return widened * lax.rsqrt(lax.optimization_barrier(jnp.mean(widened * widened, axis=-1, keepdims=True)) + EPS) * gain_row.astype(jnp.float32)

def rotate(vectors, lengths):
    half_dim = vectors.shape[-1] // 2
    frequency = THETA ** (-jnp.arange(half_dim, dtype=jnp.float32) / half_dim)
    angles = lengths.astype(jnp.float32)[:, None] * frequency[None, :]
    cosine = jnp.cos(angles)[:, None, :]
    sine_part = jnp.sin(angles)[:, None, :]
    leading = vectors[..., :half_dim]
    trailing = vectors[..., half_dim:]
    return jnp.concatenate([leading * cosine - trailing * sine_part, trailing * cosine + leading * sine_part], axis=-1)

def decay_table(head_count):
    head_order = jnp.arange(head_count, dtype=jnp.float32)
    return 1.0 - jnp.exp2(-5.0 - 7.0 * head_order / (head_count - 1))

def retain(queries, keys_new, values, out_gate, prior_state, lengths, decays):
    seq_count = queries.shape[0]
    head_count = decays.shape[0]
    layout = (seq_count, head_count, HEAD)
    rot_query = rotate(queries.astype(jnp.float32).reshape(layout), lengths)
    rot_key = rotate(keys_new.astype(jnp.float32).reshape(layout), lengths) * HEAD ** (-0.5)
    wide_values = values.astype(jnp.float32).reshape(layout)
    from_state = jnp.einsum('shd,shde->she', rot_query, prior_state, precision=lax.Precision.HIGHEST)
    self_term = lax.optimization_barrier(jnp.sum(rot_query * rot_key, axis=-1, keepdims=True))
    read_out = decays[None, :, None] * from_state + self_term * wide_values
    new_state = decays[None, :, None, None] * prior_state + rot_key[..., :, None] * wide_values[..., None, :]
    normed = read_out * lax.rsqrt(lax.optimization_barrier(jnp.mean(read_out * read_out, axis=-1, keepdims=True)) + EPS)
    gated_rows = normed.reshape(seq_count, head_count * HEAD) * jax.nn.silu(out_gate.astype(jnp.float32))
    return (gated_rows.astype(jnp.bfloat16), new_state)

def swiglu_split(inputs, w_gate, w_up, w_down):
    part_width = w_gate.shape[1] // N_TP
    running = jnp.zeros((inputs.shape[0], w_down.shape[1]), jnp.float32)
    for portion in range(N_TP):
        lower_row = portion * part_width
        gate_cols = jnp.dot(inputs, w_gate[:, lower_row:lower_row + part_width], preferred_element_type=jnp.float32)
        up_cols = jnp.dot(inputs, w_up[:, lower_row:lower_row + part_width], preferred_element_type=jnp.float32)
        hidden = (jax.nn.silu(gate_cols) * up_cols).astype(jnp.bfloat16)
        running = running + rounded(jnp.dot(hidden, w_down[lower_row:lower_row + part_width, :], preferred_element_type=jnp.float32))
    return running.astype(jnp.bfloat16)

def reference(tokens, lengths, prior_state, mix_gain, post_gain, ffn_gain, out_gain, query_weight, key_weight, value_weight, gate_weight, out_weight, routes, route_gates, expert_gate, expert_up, expert_down, shared_gate, shared_up, shared_down):
    normed = scaled_rows(tokens, mix_gain).astype(jnp.bfloat16)

    def project(weight_matrix):
        return jnp.dot(normed, weight_matrix, preferred_element_type=jnp.float32).astype(jnp.bfloat16)
    retained, new_state = retain(project(query_weight), project(key_weight), project(value_weight), project(gate_weight), prior_state, lengths, decay_table(HEADS))
    half_rows = RW // N_TP
    mixed_sum = jnp.zeros((TOKENS, D), jnp.float32)
    for portion in range(N_TP):
        lower_row = portion * half_rows
        mixed_sum = mixed_sum + rounded(jnp.dot(retained[:, lower_row:lower_row + half_rows], out_weight[lower_row:lower_row + half_rows, :], preferred_element_type=jnp.float32))
    middle = rounded(tokens.astype(jnp.float32) + scaled_rows(rounded(mixed_sum), post_gain))
    moe_in = scaled_rows(middle, ffn_gain).astype(jnp.bfloat16)
    padded_in = jnp.concatenate([moe_in, jnp.zeros((1, D), jnp.bfloat16)], axis=0)
    slot_total = N_EP * CAP

    def add_expert(running, expert_id):
        matched = routes == expert_id
        chosen = jnp.any(matched, axis=1)
        weights = lax.optimization_barrier(jnp.sum(jnp.where(matched, route_gates, jnp.zeros_like(route_gates)), axis=1))
        padded_w = jnp.concatenate([weights, jnp.zeros((1,), jnp.float32)])
        picked = jnp.nonzero(chosen, size=slot_total, fill_value=TOKENS)[0].astype(jnp.int32)
        outputs = swiglu_split(padded_in[picked], expert_gate[expert_id], expert_up[expert_id], expert_down[expert_id])
        return (running.at[picked].add(padded_w[picked][:, None] * outputs.astype(jnp.float32)), None)
    routed_all = lax.scan(add_expert, jnp.zeros((TOKENS + 1, D), jnp.float32), jnp.arange(EXPERTS, dtype=jnp.int32))[0]
    shared_out = swiglu_split(moe_in, shared_gate, shared_up, shared_down)
    mixture = shared_out.astype(jnp.float32) + routed_all[:TOKENS]
    result = (middle + scaled_rows(mixture, out_gain)).astype(jnp.bfloat16)
    return (result, new_state)
```

```python
import jax
import jax.numpy as jnp
from jax import lax
from jax.experimental import pallas as pl
from jax.experimental.pallas import tpu as pltpu
from jax.sharding import Mesh
from jax.sharding import PartitionSpec as P

HEAD = 64
HEADS = 16
EP = ("ep_0", "ep_1", "ep_2")


EPS = 1e-06
THETA = 10000.0


def sent_together(arrays, axis, dim, along):
    widths = [a.shape[along] for a in arrays]
    both = jnp.concatenate(arrays, axis=along)
    out = lax.all_gather(both, axis, axis=dim, tiled=True)
    return tuple(jnp.split(out, [sum(widths[:k]) for k in range(1, len(widths))], axis=along))


def gathered_by_axis(value, axes, dim):
    for axis in reversed(axes):
        value = lax.all_gather(value, axis, axis=dim, tiled=True)
    return value


def sent_to_all(value, axis):
    copies = jnp.broadcast_to(value, (lax.axis_size(axis), *value.shape))
    return lax.all_to_all(copies, axis, split_axis=0, concat_axis=0, tiled=True)


def of_everyone(value, axis):
    return sent_to_all(value, axis).astype(jnp.float32).sum(axis=0)


def split_up(value, dim, count):
    before, after = (value.shape[:dim], value.shape[dim + 1 :])
    return jnp.moveaxis(value.reshape(*before, count, -1, *after), dim, 0)


def summed_on_arrival(value, axis, dim):
    count = lax.axis_size(axis)
    blocks = lax.all_to_all(split_up(value, dim, count), axis, 0, 0, tiled=True)
    return jnp.sum(blocks.astype(jnp.float32), axis=0)


def gathered_total(value, axis):
    blocks = lax.all_gather(value, axis)
    return blocks.sum(axis=0)


def in_order(blocks, dim):
    shape = list(blocks.shape[1:])
    shape[dim] *= blocks.shape[0]
    return jnp.moveaxis(blocks, 0, dim).reshape(shape)


def gathered_copies(value, axis, dim):
    blocks = sent_to_all(value, axis)
    return in_order(blocks, dim)


def rounded(values):
    return lax.optimization_barrier(values.astype(jnp.bfloat16)).astype(jnp.float32)


def scaled_rows(values, gain_row):
    widened = values.astype(jnp.float32)
    return widened * lax.rsqrt(jnp.mean(widened * widened, axis=-1, keepdims=True) + EPS) * gain_row


def rotate(vectors, lengths):
    half_dim = vectors.shape[-1] // 2
    frequency = THETA ** (-jnp.arange(half_dim, dtype=jnp.float32) / half_dim)
    angles = lengths.astype(jnp.float32)[:, None] * frequency[None, :]
    cosine = jnp.cos(angles)[:, None, :]
    sine_part = jnp.sin(angles)[:, None, :]
    leading = vectors[..., :half_dim]
    trailing = vectors[..., half_dim:]
    return jnp.concatenate(
        [leading * cosine - trailing * sine_part, trailing * cosine + leading * sine_part], axis=-1
    )


def decay_table(head_count):
    head_order = jnp.arange(head_count, dtype=jnp.float32)
    return 1.0 - jnp.exp2(-5.0 - 7.0 * head_order / (head_count - 1))


def retain(queries, keys_new, values, out_gate, prior_state, lengths, decays):
    seq_count = queries.shape[0]
    head_count = decays.shape[0]
    layout = (seq_count, head_count, HEAD)
    rot_query = rotate(queries.astype(jnp.float32).reshape(layout), lengths)
    rot_key = rotate(keys_new.astype(jnp.float32).reshape(layout), lengths) * HEAD ** (-0.5)
    wide_values = values.astype(jnp.float32).reshape(layout)
    from_state = jnp.einsum("shd,shde->she", rot_query, prior_state)
    self_term = jnp.sum(rot_query * rot_key, axis=-1, keepdims=True)
    read_out = decays[None, :, None] * from_state + self_term * wide_values
    new_state = (
        decays[None, :, None, None] * prior_state
        + rot_key[..., :, None] * wide_values[..., None, :]
    )
    normed = read_out * lax.rsqrt(jnp.mean(read_out * read_out, axis=-1, keepdims=True) + EPS)
    gated_rows = normed.reshape(seq_count, head_count * HEAD) * jax.nn.silu(
        out_gate.astype(jnp.float32)
    )
    return (gated_rows.astype(jnp.bfloat16), new_state)


MESH = pl.DeviceIdType.MESH
NZ, NY, NX, NG = 8, 4, 4, 16
BF16 = jnp.bfloat16


def place():
    z, y, x, c = (lax.axis_index(name) for name in ("ep_0", "ep_1", "ep_2", "tp"))
    return z, y * NX + x, c


def device(z, g, c):
    return (z, g // NX, g % NX, c)


def remote(src, dst, send_sem, recv_sem, target):
    return pltpu.make_async_remote_copy(
        src_ref=src,
        dst_ref=dst,
        send_sem=send_sem,
        recv_sem=recv_sem,
        device_id=target,
        device_id_type=MESH,
    )


def each(low, high, body):
    def step(i, carry):
        body(i)
        return carry

    lax.fori_loop(low, high, step, 0)


def greet(z, g, c):
    barrier = pltpu.get_barrier_semaphore()

    def in_plane(i):
        pl.semaphore_signal(
            barrier, inc=1, device_id=device(z, (g + i) % NG, c), device_id_type=MESH
        )

    def in_column(j):
        other = (z * 2 + c + j) % (2 * NZ)
        pl.semaphore_signal(
            barrier, inc=1, device_id=device(other // 2, g, other % 2), device_id_type=MESH
        )

    each(1, NG, in_plane)
    each(1, 2 * NZ, in_column)
    return barrier


def project_kernel(
    tokens_ref, gain_ref, wsrc_ref, wot_ref, out_ref, wo_ref,
    tbuf, abuf, wbuf, zbuf, xsend, xbuf, osend,
    t_s, t_r, a_s, a_r, b_s, b_r, c_s, c_r, d_s, d_r, x_s, x_r, o_s, o_r, l_s,
):
    z, g, c = place()
    barrier = greet(z, g, c)
    half = tbuf.shape[-1]
    wide = tokens_ref[...].astype(jnp.float32)
    scale = lax.rsqrt(jnp.mean(wide * wide, axis=-1, keepdims=True) + EPS)
    cols = pl.ds(pl.multiple_of(c * half, 128), half)
    part = tokens_ref[:, cols].astype(jnp.float32)
    tbuf[pl.ds(g, 1)] = (part * scale * gain_ref[:, cols]).astype(BF16)[None]
    pl.semaphore_wait(barrier, NG - 1 + 2 * NZ - 1)

    def plane_copy(src, dst, send, recv, i):
        other = (g + i) % NG
        return remote(src(other), dst(g), send.at[other], recv.at[g], device(z, other, c))

    def plane_recv(src, dst, send, recv, i):
        other = (g + i) % NG
        return remote(src(other), dst(other), send.at[other], recv.at[other], device(z, other, c))

    def a_args():
        return (lambda k: wsrc_ref.at[k], lambda k: abuf.at[k], a_s, a_r)

    def t_args():
        return (lambda k: tbuf.at[g], lambda k: tbuf.at[k], t_s, t_r)

    def o_args():
        return (lambda k: osend.at[k], lambda k: out_ref.at[k], o_s, o_r)

    each(1, NG, lambda i: plane_copy(*a_args(), i).start())
    own_a = pltpu.make_async_copy(wsrc_ref.at[g], abuf.at[g], l_s.at[0])
    own_a.start()

    def c_copy(j, recv):
        other = (z + j) % NZ
        slot = other if recv else z
        return remote(wot_ref, zbuf.at[slot], c_s.at[other], c_r.at[slot], device(other, g, c))

    each(1, NG, lambda i: plane_copy(*t_args(), i).start())
    each(1, NZ, lambda j: c_copy(j, False).start())
    own_z = pltpu.make_async_copy(wot_ref, zbuf.at[z], l_s.at[1])
    own_z.start()

    each(1, NG, lambda i: plane_recv(*a_args(), i).wait_recv())
    own_a.wait()
    b_core = z // (NZ // 2)

    def b_copy(j):
        other = (z + j) % NZ
        return remote(
            abuf, wbuf.at[c, z % 4], b_s.at[j], b_r.at[c, z % 4], device(other, g, b_core)
        )

    each(1, NZ, lambda j: b_copy(j).start())

    @pl.when(b_core == c)
    def _():
        pltpu.make_async_copy(abuf, wbuf.at[c, z % 4], b_r.at[c, z % 4]).start()

    @pl.when(b_core != c)
    def _():
        b_copy(0).start()

    each(1, NZ, lambda j: c_copy(j, True).wait_recv())
    own_z.wait()
    to_half = g // (NG // 2)

    def d_copy(k):
        other = 2 * k + to_half
        return other, remote(
            zbuf.at[k], wo_ref.at[g % 8], d_s.at[k], d_r.at[g % 8], device(z, other, c)
        )

    def d_start(k):
        other, copy = d_copy(k)

        @pl.when(other == g)
        def _():
            pltpu.make_async_copy(zbuf.at[k], wo_ref.at[g % 8], d_r.at[g % 8]).start()

        @pl.when(other != g)
        def _():
            copy.start()

    each(0, NZ, d_start)

    each(1, NG, lambda i: plane_recv(*t_args(), i).wait_recv())

    def b_wait(j):
        pltpu.make_async_copy(abuf, wbuf.at[j // 4, j % 4], b_r.at[j // 4, j % 4]).wait()

    each(0, NZ, b_wait)
    rows = NG * tbuf.shape[1]
    normed = tbuf[...].reshape(rows, half)

    def weights(k):
        return wbuf[pl.ds(k, 1)].reshape(half, 128)

    xsend[...] = jnp.dot(normed, weights(1 - c), preferred_element_type=jnp.float32)
    swap = remote(xsend, xbuf, x_s, x_r, device(z, g, 1 - c))
    swap.start()
    mine = jnp.dot(normed, weights(c), preferred_element_type=jnp.float32)
    swap.wait_recv()
    osend[...] = (mine + xbuf[...]).astype(BF16).reshape(osend.shape)
    each(1, NG, lambda i: plane_copy(*o_args(), i).start())
    own_o = pltpu.make_async_copy(osend.at[g], out_ref.at[g], l_s.at[2])
    own_o.start()

    def d_wait(k):
        pltpu.make_async_copy(zbuf.at[k], wo_ref.at[k], d_r.at[k]).wait()

    each(0, NZ, d_wait)
    each(1, NG, lambda i: plane_recv(*o_args(), i).wait_recv())
    own_o.wait()
    for args in (a_args(), t_args(), o_args()):
        each(1, NG, lambda i, args=args: plane_copy(*args, i).wait_send())
    each(1, NZ, lambda j: c_copy(j, False).wait_send())
    each(1, NZ, lambda j: b_copy(j).wait_send())

    @pl.when(b_core != c)
    def _():
        b_copy(0).wait_send()

    def d_sent(k):
        other, copy = d_copy(k)

        @pl.when(other != g)
        def _():
            copy.wait_send()

    each(0, NZ, d_sent)
    swap.wait_send()


def project(tokens, mix_gain, weights, out_weight):
    seq, width = tokens.shape
    wsrc = jnp.concatenate(weights, axis=1).reshape(seq, NG, 128).transpose(1, 0, 2)
    dma = pltpu.SemaphoreType.DMA
    return pl.pallas_call(
        project_kernel,
        out_shape=(
            jax.ShapeDtypeStruct((NG, seq, 128), BF16),
            jax.ShapeDtypeStruct((8, 16, 512), BF16),
        ),
        in_specs=[pl.BlockSpec(memory_space=pltpu.VMEM)] * 4,
        out_specs=(pl.BlockSpec(memory_space=pltpu.VMEM),) * 2,
        scratch_shapes=[
            pltpu.VMEM((NG, seq, width // 2), BF16),
            pltpu.VMEM((NG, 16, 128), BF16),
            pltpu.VMEM((2, 4, NG, 16, 128), BF16),
            pltpu.VMEM((8, 16, 512), BF16),
            pltpu.VMEM((NG * seq, 128), jnp.float32),
            pltpu.VMEM((NG * seq, 128), jnp.float32),
            pltpu.VMEM((NG, seq, 128), BF16),
            dma((NG,)), dma((NG,)), dma((NG,)), dma((NG,)),
            dma((NZ,)), dma((2, 4)), dma((NZ,)), dma((NZ,)), dma((NZ,)), dma((NZ,)),
            dma, dma, dma((NG,)), dma((NG,)), dma((3,)),
        ],
        compiler_params=pltpu.CompilerParams(collective_id=0, has_side_effects=True),
        name="project",
    )(tokens, mix_gain[None], wsrc, out_weight.T)


def on_device(
    tokens,
    lengths,
    prior_state,
    mix_gain,
    post_gain,
    ffn_gain,
    out_gain,
    query_weight,
    key_weight,
    value_weight,
    gate_weight,
    out_weight,
    routes,
    route_gates,
    expert_gate,
    expert_up,
    expert_down,
    shared_gate,
    shared_up,
    shared_down,
):
    seq_here = tokens.shape[0]
    model_width = tokens.shape[1]
    local_cols = query_weight.shape[1]
    blocks, wo_blocks = project(
        tokens, mix_gain, (query_weight, key_weight, value_weight, gate_weight), out_weight
    )
    queries, keys_new, values, out_gate = (
        blocks[4 * k : 4 * k + 4].transpose(1, 0, 2).reshape(seq_here, local_cols) for k in range(4)
    )
    heads_here = local_cols // HEAD
    decays = lax.dynamic_slice_in_dim(
        decay_table(HEADS), lax.axis_index("tp") * heads_here, heads_here, 0
    )
    retained, new_state = retain(queries, keys_new, values, out_gate, prior_state, lengths, decays)
    partial_mix = jnp.dot(
        retained, gathered_by_axis(out_weight, EP, 1), preferred_element_type=jnp.float32
    )
    mixed_sum = rounded(
        of_everyone(rounded(partial_mix).astype(jnp.bfloat16), "tp").astype(jnp.float32)
    )
    middle = rounded(tokens.astype(jnp.float32) + scaled_rows(mixed_sum, post_gain))
    moe_in = scaled_rows(middle, ffn_gain).astype(jnp.bfloat16)
    experts_all = lax.axis_size(EP)
    topk_here = routes.shape[1]
    capacity = seq_here * topk_here // experts_all + 2
    slot_count = experts_all * capacity
    flat_routes = routes.reshape(-1)
    onehot = (flat_routes[:, None] == jnp.arange(experts_all, dtype=jnp.int32)[None, :]).astype(
        jnp.int32
    )
    earlier = jnp.cumsum(onehot, axis=0) - onehot
    ranks = jnp.sum(earlier * onehot, axis=1)
    slot_ids = flat_routes * capacity + ranks
    placing = (jnp.arange(slot_count, dtype=jnp.int32)[:, None] == slot_ids[None, :]).reshape(
        slot_count, seq_here, topk_here
    )
    dispatch_rows = jnp.any(placing, axis=2).astype(jnp.bfloat16)
    combine = jnp.sum(
        jnp.where(placing, route_gates[None, :, :], jnp.zeros((), jnp.float32)), axis=2
    ).T
    outgoing = jnp.dot(dispatch_rows, moe_in, preferred_element_type=jnp.float32).astype(
        jnp.bfloat16
    )
    outgoing = outgoing.reshape(experts_all, capacity, model_width)
    gate_local = expert_gate[0]
    up_local = expert_up[0]
    down_local = expert_down[0]
    arrived = lax.all_to_all(outgoing, EP, split_axis=0, concat_axis=0, tiled=True)
    sources = arrived.shape[0]
    held_slots = arrived.shape[1]
    flat_in = arrived.reshape(sources * held_slots, model_width)
    hidden = (
        jax.nn.silu(jnp.dot(flat_in, gate_local, preferred_element_type=jnp.float32))
        * jnp.dot(flat_in, up_local, preferred_element_type=jnp.float32)
    ).astype(jnp.bfloat16)
    partial_out = rounded(jnp.dot(hidden, down_local, preferred_element_type=jnp.float32))
    expert_sum = summed_on_arrival(partial_out.astype(jnp.bfloat16), "tp", 1).astype(jnp.bfloat16)
    returned = lax.all_to_all(
        expert_sum.reshape(sources, held_slots, -1), EP, split_axis=0, concat_axis=0, tiled=True
    )
    back_rows = returned.reshape(slot_count, -1).astype(jnp.float32)
    routed = jnp.dot(combine, back_rows)
    shared_hidden = (
        jax.nn.silu(jnp.dot(moe_in, shared_gate, preferred_element_type=jnp.float32))
        * jnp.dot(moe_in, shared_up, preferred_element_type=jnp.float32)
    ).astype(jnp.bfloat16)
    shared_part = rounded(jnp.dot(shared_hidden, shared_down, preferred_element_type=jnp.float32))
    shared_out = summed_on_arrival(shared_part.astype(jnp.bfloat16), "tp", 1).astype(jnp.bfloat16)
    mixture = shared_out.astype(jnp.float32) + routed
    squares = gathered_total(jnp.sum(mixture * mixture, axis=1, keepdims=True), "tp")
    half_cols = mixture.shape[1]
    offset = lax.axis_index("tp") * half_cols
    gain_part = lax.dynamic_slice_in_dim(out_gain, offset, half_cols, 0)
    middle_part = lax.dynamic_slice_in_dim(middle, offset, half_cols, 1)
    scale_rows = lax.rsqrt(squares / model_width + EPS)
    half_result = (middle_part + mixture * scale_rows * gain_part).astype(jnp.bfloat16)
    result = gathered_copies(half_result, "tp", 1)
    return (result, new_state)


def solution(mesh):
    finer = Mesh(mesh.devices.reshape(8, 4, 4, mesh.shape["tp"]), ("ep_0", "ep_1", "ep_2", "tp"))
    in_specs = (
        P(EP, None),
        P(EP),
        P(EP, "tp", None, None),
        P(),
        P(),
        P(),
        P(),
        P(EP, "tp"),
        P(EP, "tp"),
        P(EP, "tp"),
        P(EP, "tp"),
        P("tp", EP),
        P(EP, None),
        P(EP, None),
        P(EP, None, "tp"),
        P(EP, None, "tp"),
        P(EP, "tp", None),
        P(None, "tp"),
        P(None, "tp"),
        P("tp", None),
    )
    out_specs = (P(EP, None), P(EP, "tp", None, None))
    return jax.shard_map(
        on_device, mesh=finer, in_specs=in_specs, out_specs=out_specs, check_vma=False
    )
```

```python
import jax
import jax.numpy as jnp
import numpy as np
from jax import lax
from jax.experimental import pallas as pl
from jax.experimental.pallas import tpu as pltpu
from jax.sharding import Mesh
from jax.sharding import PartitionSpec as P

HEAD = 64
HEADS = 16
EP = ("ep_0", "ep_1", "ep_2")
EPS = 1e-06
THETA = 10000.0
MESH = pl.DeviceIdType.MESH
NZ, NY, NX, NG = 8, 4, 4, 16
BF16 = jnp.bfloat16
F32 = jnp.float32


def place():
    z, y, x, c = (lax.axis_index(name) for name in ("ep_0", "ep_1", "ep_2", "tp"))
    return z, y * NX + x, c


def device(z, g, c):
    return (z, g // NX, g % NX, c)


def remote(src, dst, send_sem, recv_sem, target):
    return pltpu.make_async_remote_copy(
        src_ref=src,
        dst_ref=dst,
        send_sem=send_sem,
        recv_sem=recv_sem,
        device_id=target,
        device_id_type=MESH,
    )


def each(low, high, body):
    def step(i, carry):
        body(i)
        return carry

    lax.fori_loop(low, high, step, 0)


def dot(a, b, dims=((1,), (0,))):
    return lax.dot_general(a, b, (dims, ((), ())), preferred_element_type=F32)


def wide_rows(blocks):
    rows = blocks.shape[0] * blocks.shape[2]
    return jnp.concatenate(
        [blocks[:, k].reshape(rows, 128) for k in range(blocks.shape[1])], axis=1
    )


def row_scale(blocks):
    count = blocks.shape[0] * blocks.shape[2]
    total = jnp.sum(jnp.sum(blocks * blocks, axis=0), axis=-1, keepdims=True)
    return lax.rsqrt(total / count + EPS)[None]


class Group:
    def __init__(self, me, size, at, src, dst, send, recv):
        self.me, self.size, self.at, self.src, self.dst = me, size, at, src, dst
        self.send, self.recv = send, recv

    def out(self, i):
        k = (self.me + i) % self.size
        return remote(
            self.src(k), self.dst(self.me), self.send.at[k], self.recv.at[self.me], self.at(k)
        )

    def come(self, i):
        k = (self.me + i) % self.size
        return remote(
            self.src(k), self.dst(k), self.send.at[k], self.recv.at[k], self.at(k)
        )

    def start(self):
        each(1, self.size, lambda i: self.out(i).start())

    def wait(self):
        each(1, self.size, lambda i: self.come(i).wait_recv())

    def drain(self):
        each(1, self.size, lambda i: self.out(i).wait_send())


def layer_kernel(
    tokens_ref, mix_ref, post_ref, ffn_ref, outg_ref, wsrc_ref, wot_ref, cos_ref, sin_ref, dec_ref, rt_ref,
    state_hbm, eg_hbm, eu_hbm, ed_hbm, sg_hbm, su_hbm, sd_hbm,
    result_ref, new_hbm,
    state, eg, eu, ed, sg, su, sd,
    tbuf, abuf, wbuf, zbuf, wo, xsend, xbuf, osend, obuf, qbuf, onehot, comb_hi, comb_lo,
    kt, vsc, fs, rbuf, psend, pbuf, middle, mo, mbuf, shs, shb, ysend, ebuf, dsend, dbuf, ret, back,
    csend, cbuf, mixs, mixb,
    l_s, w_s, a_s, a_r, t_s, t_r, b_s, b_r, c_s, c_r, d_s, d_r, q_s, q_r, o_s, o_r, r_s, r_r,
    p_s, p_r, m_s, m_r, y_s, y_r, f_s, f_r, g_s, g_r, h_s, h_r, x_s, x_r,
):
    z, g, c = place()
    loads = [
        pltpu.make_async_copy(src, dst, w_s.at[i])
        for i, (src, dst) in enumerate(
            ((state_hbm, state), (sg_hbm, sg), (su_hbm, su), (sd_hbm, sd),
             (eg_hbm, eg), (eu_hbm, eu), (ed_hbm, ed))
        )
    ]
    barrier = pltpu.get_barrier_semaphore()

    def greet_plane(i):
        other = (g * 2 + c + i) % (2 * NG)
        pl.semaphore_signal(
            barrier, inc=1, device_id=device(z, other // 2, other % 2), device_id_type=MESH
        )

    def greet_column(i):
        other = (z + 1 + i // 2) % NZ
        pl.semaphore_signal(
            barrier, inc=1, device_id=device(other, g, i % 2), device_id_type=MESH
        )

    each(1, 2 * NG, greet_plane)
    each(0, 2 * NZ - 2, greet_column)
    for load in loads:
        load.start()

    half = tbuf.shape[-1]
    wide = tokens_ref[...].astype(F32)
    scale = lax.rsqrt(jnp.mean(wide * wide, axis=-1, keepdims=True) + EPS)
    cols = pl.ds(pl.multiple_of(c * half, 128), half)
    part = tokens_ref[:, cols].astype(F32)
    tbuf[pl.ds(g, 1)] = (part * scale * mix_ref[:, cols]).astype(BF16)[None]
    pl.semaphore_wait(barrier, 2 * NG - 1 + 2 * NZ - 2)

    def plane(src, dst, send, recv):
        return Group(g, NG, lambda k: device(z, k, c), src, dst, send, recv)

    def column(src, dst, send, recv):
        return Group(z, NZ, lambda k: device(k, g, c), src, dst, send, recv)

    ga = plane(lambda k: wsrc_ref.at[k], lambda k: abuf.at[k], a_s, a_r)
    gt = plane(lambda k: tbuf.at[g], lambda k: tbuf.at[k], t_s, t_r)
    gc = column(lambda k: wot_ref, lambda k: zbuf.at[k], c_s, c_r)
    gq = column(lambda k: rt_ref, lambda k: qbuf.at[k], q_s, q_r)
    ga.start()
    own_a = pltpu.make_async_copy(wsrc_ref.at[g], abuf.at[g], l_s.at[0])
    own_a.start()
    gt.start()
    gc.start()
    gq.start()
    own_z = pltpu.make_async_copy(wot_ref, zbuf.at[z], l_s.at[1])
    own_z.start()
    qbuf[pl.ds(z, 1)] = rt_ref[...][None]

    ga.wait()
    own_a.wait()
    b_core = z // (NZ // 2)

    def b_copy(j):
        other = (z + j) % NZ
        return remote(
            abuf, wbuf.at[c, z % 4], b_s.at[j], b_r.at[c, z % 4], device(other, g, b_core)
        )

    each(1, NZ, lambda j: b_copy(j).start())

    @pl.when(b_core == c)
    def _():
        pltpu.make_async_copy(abuf, wbuf.at[c, z % 4], b_r.at[c, z % 4]).start()

    @pl.when(b_core != c)
    def _():
        b_copy(0).start()

    gc.wait()
    own_z.wait()
    to_half = g // (NG // 2)

    def d_copy(k):
        other = 2 * k + to_half
        return other, remote(
            zbuf.at[k], wo.at[g % 8], d_s.at[k], d_r.at[g % 8], device(z, other, c)
        )

    def d_start(k):
        other, copy = d_copy(k)

        @pl.when(other == g)
        def _():
            pltpu.make_async_copy(zbuf.at[k], wo.at[g % 8], d_r.at[g % 8]).start()

        @pl.when(other != g)
        def _():
            copy.start()

    each(0, NZ, d_start)

    gq.wait()
    routing = qbuf[...].reshape(NZ * 16, 128)
    slots = 16 * NG
    row_z = lax.broadcasted_iota(jnp.int32, (NZ * 16, slots), 0) // 16
    lane = lax.broadcasted_iota(jnp.int32, (NZ * 16, slots), 1)
    slot_id = ((z * NG + lane // 16) * 2 + lane % 2).astype(F32)
    same_z = row_z == (lane % 16) // 2
    named = jnp.zeros((NZ * 16, slots), F32)
    weight = jnp.zeros((NZ * 16, slots), F32)
    for k in range(6):
        hit = jnp.logical_and(routing[:, k : k + 1] == slot_id, same_z)
        named = named + jnp.where(hit, 1.0, 0.0)
        weight = weight + jnp.where(hit, routing[:, 8 + k : 9 + k], 0.0)
    onehot[...] = named.T.astype(BF16)
    upper = weight.astype(BF16)
    comb_hi[...] = upper
    comb_lo[...] = (weight - upper.astype(F32)).astype(BF16)

    gt.wait()

    def b_wait(j):
        pltpu.make_async_copy(abuf, wbuf.at[j // 4, j % 4], b_r.at[j // 4, j % 4]).wait()

    each(0, NZ, b_wait)
    rows = NG * tbuf.shape[1]
    normed = tbuf[...].reshape(rows, half)

    def weights(k):
        return wbuf[pl.ds(k, 1)].reshape(half, 128)

    xsend[...] = dot(normed, weights(1 - c))
    swap = remote(xsend, xbuf, x_s.at[0], x_r.at[0], device(z, g, 1 - c))
    swap.start()
    mine = dot(normed, weights(c))
    swap.wait_recv()
    osend[...] = (mine + xbuf[...]).astype(BF16).reshape(osend.shape)
    go = plane(lambda k: osend.at[k], lambda k: obuf.at[k], o_s, o_r)
    go.start()
    obuf[pl.ds(g, 1)] = osend[pl.ds(g, 1)]
    loads[0].wait()
    fs[...] = jnp.zeros_like(fs)
    go.wait()

    low_half = lax.broadcasted_iota(jnp.int32, (16, 128), 1) < 64
    first = lax.broadcasted_iota(jnp.int32, (16, 128), 1) % 64 < 32

    def rotate(v):
        other = jnp.where(first, pltpu.roll(v, 96, 1), pltpu.roll(v, 32, 1))
        return v * cos_ref[...] + other * sin_ref[...]

    def by_head(v):
        low = jnp.sum(jnp.where(low_half, v, 0.0), axis=-1, keepdims=True)
        high = jnp.sum(jnp.where(low_half, 0.0, v), axis=-1, keepdims=True)
        return jnp.where(low_half, low, high)

    def read_pair(hp):
        def block(k):
            return obuf[pl.ds(4 * k + hp, 1)][0].astype(F32)

        query = rotate(block(0))
        key = rotate(block(1)) * HEAD ** (-0.5)
        value = block(2)
        query_t = query.T
        kt[pl.ds(hp, 1)] = key.T[None]
        vsc[pl.ds(2 * hp, 1)] = value[None]
        vsc[pl.ds(2 * hp + 1, 1)] = pltpu.roll(value, 64, 1)[None]
        for h in range(2):
            for s in range(16):
                held = state[s, pl.ds(2 * hp + h, 1)][0]
                column_q = query_t[h * 64 : (h + 1) * 64, s : s + 1]
                fs[h, s : s + 1, 0:64] = jnp.sum(column_q * held, axis=0, keepdims=True)
        from_state = jnp.where(low_half, fs[0], pltpu.roll(fs[1], 64, 1))
        decay = jnp.where(
            low_half[0:1], dec_ref[c, pl.ds(2 * hp, 1)], dec_ref[c, pl.ds(2 * hp + 1, 1)]
        )
        read = decay * from_state + by_head(query * key) * value
        read = read * lax.rsqrt(by_head(read * read) / HEAD + EPS)
        rbuf[pl.ds(g, 1), pl.ds(hp, 1)] = (read * jax.nn.silu(block(3))).astype(BF16)[None, None]

    each(0, 4, read_pair)
    gr = plane(lambda k: rbuf.at[g], lambda k: rbuf.at[k], r_s, r_r)
    gr.start()

    def update_pair(hp):
        keys = kt[pl.ds(hp, 1)][0]
        for h in range(2):
            decay = dec_ref[c, pl.ds(2 * hp + h, 1)][:, 0:64]
            value = vsc[pl.ds(2 * hp + h, 1)][0]
            for s in range(16):
                held = state[s, pl.ds(2 * hp + h, 1)][0]
                column_k = keys[h * 64 : (h + 1) * 64, s : s + 1]
                state[s, pl.ds(2 * hp + h, 1)] = (
                    decay * held + column_k * value[s : s + 1, 0:64]
                )[None]

    each(0, 4, update_pair)
    store = pltpu.make_async_copy(state, new_hbm, w_s.at[7])
    store.start()

    def d_wait(k):
        pltpu.make_async_copy(zbuf.at[k], wo.at[k], d_r.at[k]).wait()

    each(0, NZ, d_wait)
    gr.wait()

    partial = dot(wide_rows(rbuf[...]), wo[...].reshape(128, 512), ((1,), (1,)))
    psend[...] = partial.astype(BF16).reshape(psend.shape)
    gp = [
        plane(lambda k: psend.at[k], lambda k: pbuf.at[c, k], p_s.at[0], p_r.at[c]),
    ]
    gp[0].start()
    gp_other = Group(
        g, NG, lambda k: device(z, k, 1 - c), lambda k: psend.at[k], lambda k: pbuf.at[c, k],
        p_s.at[1], p_r.at[c],
    )
    each(0, NG, lambda i: gp_other.out(i).start())
    pbuf[pl.ds(c, 1), pl.ds(g, 1)] = psend[pl.ds(g, 1)][None]
    gp[0].wait()
    gp_from = Group(
        g, NG, lambda k: device(z, k, 1 - c), lambda k: psend.at[k], lambda k: pbuf.at[1 - c, k],
        p_s.at[1], p_r.at[1 - c],
    )
    each(0, NG, lambda i: gp_from.come(i).wait_recv())
    mixed = (pbuf[0].astype(F32) + pbuf[1].astype(F32)).astype(BF16).astype(F32)
    tok = jnp.stack([tokens_ref[:, k * 128 : (k + 1) * 128] for k in range(NG)]).astype(F32)
    mid = (tok + mixed * row_scale(mixed) * post_ref[...]).astype(BF16)
    middle[...] = mid
    mid = mid.astype(F32)
    mo[...] = (mid * row_scale(mid) * ffn_ref[...]).astype(BF16)

    own_blocks = pl.ds(pl.multiple_of(c * 8, 8), 8)
    mbuf[pl.ds(z, 1)] = mo[own_blocks][None]
    gm = column(lambda k: mbuf.at[z], lambda k: mbuf.at[k], m_s, m_r)
    gm.start()
    for load in loads[1:4]:
        load.wait()
    rows_in = wide_rows(mo[...][None])
    shared_hidden = (jax.nn.silu(dot(rows_in, sg[...])) * dot(rows_in, su[...])).astype(BF16)
    shared_part = dot(shared_hidden, sd[...]).astype(BF16)
    parts = jnp.stack([shared_part[:, k * 128 : (k + 1) * 128] for k in range(NG)])
    shs[...] = parts.reshape(shs.shape)
    share = remote(shs.at[1 - c], shb, x_s.at[1], x_r.at[1], device(z, g, 1 - c))
    share.start()
    for load in loads[4:]:
        load.wait()
    gm.wait()
    sorted_rows = dot(onehot[...], wide_rows(mbuf[...])).astype(BF16)
    for k in range(8):
        ysend[:, k] = sorted_rows[:, k * 128 : (k + 1) * 128].reshape(NG, 16, 128)
    gy = plane(lambda k: ysend.at[k], lambda k: ebuf.at[c, k], y_s, y_r)
    gy.start()
    ebuf[pl.ds(c, 1), pl.ds(g, 1)] = ysend[pl.ds(g, 1)][None]

    def forward(half_from, k):
        return remote(
            ebuf.at[half_from, k], ebuf.at[half_from, k], f_s.at[k], f_r.at[k], device(z, g, 1 - c)
        )

    forward(c, g).start()

    def relay(i):
        gy.come(i).wait_recv()
        forward(c, (g + i) % NG).start()

    each(1, NG, relay)

    def expert_in(k):
        blocks = wide_rows(ebuf[pl.ds(k, 1)][0])
        rows_of = pl.ds(pl.multiple_of(k * half, 128), half)
        return dot(blocks, eg[0, rows_of]), dot(blocks, eu[0, rows_of])

    gate_c, up_c = expert_in(c)
    each(0, NG, lambda k: forward(1 - c, k).wait_recv())
    gate_o, up_o = expert_in(1 - c)
    hidden = (jax.nn.silu(gate_c + gate_o) * (up_c + up_o)).astype(BF16)

    def down(k):
        out = dot(hidden, ed[0, :, pl.ds(pl.multiple_of(k * half, 128), half)]).astype(BF16)
        return [out[:, j * 128 : (j + 1) * 128].reshape(NG, 16, 128) for j in range(8)]

    for j, block in enumerate(down(1 - c)):
        dsend[:, j] = block
    give = remote(dsend, dbuf, x_s.at[2], x_r.at[2], device(z, g, 1 - c))
    give.start()
    kept = down(c)
    give.wait_recv()
    for j in range(8):
        ret[:, j] = (kept[j].astype(F32) + dbuf[:, j].astype(F32)).astype(BF16)
    gg = plane(lambda k: ret.at[k], lambda k: back.at[k], g_s, g_r)
    gg.start()
    back[pl.ds(g, 1)] = ret[pl.ds(g, 1)]
    share.wait_recv()
    shared_out = (shs[pl.ds(c, 1)][0].astype(F32) + shb[...].astype(F32)).astype(BF16).astype(F32)
    gg.wait()

    answers = wide_rows(back[...])
    sums = (dot(comb_hi[...], answers) + dot(comb_lo[...], answers)).astype(BF16)
    for k in range(8):
        csend[:, k] = sums[:, k * 128 : (k + 1) * 128].reshape(NZ, 16, 128)
    gh = column(lambda k: csend.at[k], lambda k: cbuf.at[k], h_s, h_r)
    gh.start()
    cbuf[pl.ds(z, 1)] = csend[pl.ds(z, 1)]
    gh.wait()
    mixs[...] = shared_out + jnp.sum(cbuf[...].astype(F32), axis=0)
    last = remote(mixs, mixb, x_s.at[3], x_r.at[3], device(z, g, 1 - c))
    last.start()
    last.wait_recv()
    first_half = jnp.where(c == 0, mixs[...], mixb[...])
    second_half = jnp.where(c == 0, mixb[...], mixs[...])
    mixture = jnp.concatenate([first_half, second_half], axis=0)
    final = (middle[...].astype(F32) + mixture * row_scale(mixture) * outg_ref[...]).astype(BF16)
    for k in range(NG):
        result_ref[:, k * 128 : (k + 1) * 128] = final[k]

    for group in (ga, gt, gc, gq, go, gr, gp[0], gm, gy, gg, gh):
        group.drain()
    each(0, NG, lambda i: gp_other.out(i).wait_send())
    each(1, NZ, lambda j: b_copy(j).wait_send())

    @pl.when(b_core != c)
    def _():
        b_copy(0).wait_send()

    def d_sent(k):
        other, copy = d_copy(k)

        @pl.when(other != g)
        def _():
            copy.wait_send()

    each(0, NZ, d_sent)
    each(0, NG, lambda k: forward(c, k).wait_send())
    for copy in (swap, share, give, last):
        copy.wait_send()
    store.wait()


def decay_table(head_count):
    head_order = np.arange(head_count, dtype=np.float32)
    decays = (1.0 - np.exp2(-5.0 - 7.0 * head_order / (head_count - 1))).astype(np.float32)
    return np.broadcast_to(decays.reshape(2, -1, 1), (2, head_count // 2, 128))


def on_device(
    tokens, lengths, prior_state, mix_gain, post_gain, ffn_gain, out_gain,
    query_weight, key_weight, value_weight, gate_weight, out_weight, routes, route_gates,
    expert_gate, expert_up, expert_down, shared_gate, shared_up, shared_down,
):
    seq, width = tokens.shape
    half_dim = HEAD // 2
    frequency = THETA ** (-jnp.arange(half_dim, dtype=F32) / half_dim)
    angles = lengths.astype(F32)[:, None] * frequency[None, :]
    cosine, sine = jnp.cos(angles), jnp.sin(angles)
    cos_table = jnp.concatenate([cosine] * 4, axis=1)
    sin_table = jnp.concatenate([-sine, sine] * 2, axis=1)
    earlier = jnp.arange(seq)[None, None, :, None] < jnp.arange(seq)[:, None, None, None]
    same = routes[:, :, None, None] == routes[None, None]
    rank = jnp.any(jnp.logical_and(same, earlier), axis=(2, 3)).astype(jnp.int32)
    slot = (routes * 2 + rank).astype(F32)
    gap = jnp.zeros((seq, 2), F32)
    table = jnp.concatenate([slot, gap, route_gates, jnp.zeros((seq, 114), F32)], axis=1)
    wsrc = jnp.concatenate((query_weight, key_weight, value_weight, gate_weight), axis=1)
    wsrc = wsrc.reshape(seq, NG, 128).transpose(1, 0, 2)
    dma = pltpu.SemaphoreType.DMA
    blocks = pltpu.VMEM((NG, 16, 128), BF16)
    halves = pltpu.VMEM((NG, 8, 16, 128), BF16)
    square = pltpu.VMEM((NG * seq, 128), F32)
    vmem = pl.BlockSpec(memory_space=pltpu.VMEM)
    anywhere = pl.BlockSpec(memory_space=pl.ANY)
    big = (prior_state, expert_gate, expert_up, expert_down, shared_gate, shared_up, shared_down)
    plane_sems, column_sems = dma((NG,)), dma((NZ,))
    return pl.pallas_call(
        layer_kernel,
        out_shape=(
            jax.ShapeDtypeStruct((seq, width), BF16),
            jax.ShapeDtypeStruct(prior_state.shape, F32),
        ),
        in_specs=[vmem] * 11 + [anywhere] * 7,
        out_specs=(vmem, anywhere),
        scratch_shapes=[
            *(pltpu.VMEM(array.shape, array.dtype) for array in big),
            pltpu.VMEM((NG, seq, width // 2), BF16),
            blocks,
            pltpu.VMEM((2, 4, NG, 16, 128), BF16),
            pltpu.VMEM((8, 16, 512), BF16),
            pltpu.VMEM((8, 16, 512), BF16),
            square,
            square,
            blocks,
            blocks,
            pltpu.VMEM((NZ, 16, 128), F32),
            pltpu.VMEM((16 * NG, 16 * NZ), BF16),
            pltpu.VMEM((16 * NZ, 16 * NG), BF16),
            pltpu.VMEM((16 * NZ, 16 * NG), BF16),
            pltpu.VMEM((4, 128, 16), F32),
            pltpu.VMEM((8, 16, 128), F32),
            pltpu.VMEM((2, 16, 128), F32),
            pltpu.VMEM((NG, 4, 16, 128), BF16),
            blocks,
            pltpu.VMEM((2, NG, 16, 128), BF16),
            blocks,
            blocks,
            pltpu.VMEM((NZ, 8, 16, 128), BF16),
            pltpu.VMEM((2, 8, 16, 128), BF16),
            pltpu.VMEM((8, 16, 128), BF16),
            halves,
            pltpu.VMEM((2, NG, 8, 16, 128), BF16),
            halves,
            halves,
            halves,
            halves,
            pltpu.VMEM((NZ, 8, 16, 128), BF16),
            pltpu.VMEM((NZ, 8, 16, 128), BF16),
            pltpu.VMEM((8, 16, 128), F32),
            pltpu.VMEM((8, 16, 128), F32),
            dma((2,)),
            dma((8,)),
            plane_sems, plane_sems,
            plane_sems, plane_sems,
            column_sems, dma((2, 4)),
            column_sems, column_sems,
            column_sems, column_sems,
            column_sems, column_sems,
            plane_sems, plane_sems,
            plane_sems, plane_sems,
            dma((2, NG)), dma((2, NG)),
            column_sems, column_sems,
            plane_sems, plane_sems,
            plane_sems, plane_sems,
            plane_sems, plane_sems,
            column_sems, column_sems,
            dma((4,)), dma((4,)),
        ],
        compiler_params=pltpu.CompilerParams(collective_id=0, has_side_effects=True),
        name="layer",
    )(
        tokens,
        mix_gain[None],
        *(gain.reshape(NG, 1, 128) for gain in (post_gain, ffn_gain, out_gain)),
        wsrc,
        out_weight.T,
        cos_table,
        sin_table,
        jnp.asarray(decay_table(HEADS)),
        table,
        *big,
    )


def solution(mesh):
    finer = Mesh(mesh.devices.reshape(8, 4, 4, mesh.shape["tp"]), ("ep_0", "ep_1", "ep_2", "tp"))
    in_specs = (
        P(EP, None),
        P(EP),
        P(EP, "tp", None, None),
        P(),
        P(),
        P(),
        P(),
        P(EP, "tp"),
        P(EP, "tp"),
        P(EP, "tp"),
        P(EP, "tp"),
        P("tp", EP),
        P(EP, None),
        P(EP, None),
        P(EP, None, "tp"),
        P(EP, None, "tp"),
        P(EP, "tp", None),
        P(None, "tp"),
        P(None, "tp"),
        P("tp", None),
    )
    out_specs = (P(EP, None), P(EP, "tp", None, None))
    return jax.shard_map(
        on_device, mesh=finer, in_specs=in_specs, out_specs=out_specs, check_vma=False
    )
```

```python
import jax
import jax.numpy as jnp
import numpy as np
from jax import lax
from jax.experimental import pallas as pl
from jax.experimental.pallas import tpu as pltpu
from jax.sharding import Mesh
from jax.sharding import PartitionSpec as P

HEAD = 64
HEADS = 16
EP = ("ep_0", "ep_1", "ep_2")
EPS = 1e-06
THETA = 10000.0
MESH = pl.DeviceIdType.MESH
NZ, NY, NX, NG = 8, 4, 4, 16
BF16 = jnp.bfloat16
F32 = jnp.float32


def place():
    z, y, x, c = (lax.axis_index(name) for name in ("ep_0", "ep_1", "ep_2", "tp"))
    return z, y * NX + x, c


def device(z, g, c):
    return (z, g >> 2, g & 3, c)


def remote(src, dst, send_sem, recv_sem, target):
    return pltpu.make_async_remote_copy(
        src_ref=src,
        dst_ref=dst,
        send_sem=send_sem,
        recv_sem=recv_sem,
        device_id=target,
        device_id_type=MESH,
    )


def each(low, high, body):
    def step(i, carry):
        body(i)
        return carry

    lax.fori_loop(low, high, step, 0)


def dot(a, b, dims=((1,), (0,))):
    return lax.dot_general(a, b, (dims, ((), ())), preferred_element_type=F32)


def wide_rows(blocks):
    rows = blocks.shape[0] * blocks.shape[2]
    return jnp.concatenate(
        [blocks[:, k].reshape(rows, 128) for k in range(blocks.shape[1])], axis=1
    )


def decay_of(head):
    return 1.0 - jnp.exp2(-5.0 - 7.0 * head / (HEADS - 1))


def row_scale(blocks):
    count = blocks.shape[0] * blocks.shape[2]
    total = jnp.sum(jnp.sum(blocks * blocks, axis=0), axis=-1, keepdims=True)
    return lax.rsqrt(total / count + EPS)[None]


class Group:
    def __init__(self, me, size, at, src, dst, send, recv):
        self.me, self.size, self.at, self.src, self.dst = me, size, at, src, dst
        self.send, self.recv = send, recv

    def out(self, i):
        k = (self.me + i) & (self.size - 1)
        return remote(
            self.src(k), self.dst(self.me), self.send.at[k], self.recv.at[self.me], self.at(k)
        )

    def come(self, i):
        k = (self.me + i) & (self.size - 1)
        return remote(
            self.src(k), self.dst(k), self.send.at[k], self.recv.at[k], self.at(k)
        )

    def start(self):
        each(1, self.size, lambda i: self.out(i).start())

    def wait(self):
        each(1, self.size, lambda i: self.come(i).wait_recv())

    def drain(self):
        each(1, self.size, lambda i: self.out(i).wait_send())


def layer_kernel(
    tokens_ref, lengths_ref, mix_ref, post_ref, ffn_ref, outg_ref, wq_ref, wk_ref, wv_ref, wg_ref, wot_ref,
    routes_ref, gates_ref, freq_ref,
    state_hbm, eg_hbm, eu_hbm, ed_hbm, sg_hbm, su_hbm, sd_hbm,
    result_ref, state,
    eg, eu, ed, sg, su, sd,
    wsrc, packed, rt, trig,
    tbuf, abuf, wbuf, zbuf, wo, xsend, xbuf, osend, obuf, qbuf, onehot, comb_hi, comb_lo,
    kt, vsc, fs, rbuf, psend, pbuf, middle, mo, mbuf, shs, shb, ysend, ebuf, dsend, dbuf, ret, back,
    csend, cbuf, mixs, mixb,
    l_s, w_s, a_s, a_r, t_s, t_r, b_s, n_s, b_r, c_s, c_r, d_s, d_r, q_s, q_r, o_s, o_r, r_s, r_r,
    p_s, p_r, m_s, m_r, y_s, y_r, f_s, f_r, g_s, g_r, h_s, h_r, x_s, x_r,
):
    z, g, c = place()
    loads = [
        pltpu.make_async_copy(src, dst, w_s.at[i])
        for i, (src, dst) in enumerate(
            ((state_hbm, state), (sg_hbm, sg), (su_hbm, su), (sd_hbm, sd),
             (eg_hbm, eg), (eu_hbm, eu), (ed_hbm, ed))
        )
    ]
    barrier = pltpu.get_barrier_semaphore()

    for i in range(1, 2 * NG):
        other = (g * 2 + c + i) & (2 * NG - 1)
        pl.semaphore_signal(
            barrier, inc=1, device_id=device(z, other >> 1, other & 1), device_id_type=MESH
        )
    for i in range(1, NZ):
        for core in range(2):
            pl.semaphore_signal(
                barrier, inc=1, device_id=device((z + i) & (NZ - 1), g, core), device_id_type=MESH
            )
    for load in loads:
        load.start()
    for m, w_ref in enumerate((wq_ref, wk_ref, wv_ref, wg_ref)):
        for k in range(4):
            wsrc[4 * m + k] = w_ref[:, k * 128 : (k + 1) * 128]

    half = tbuf.shape[-1]
    wide = tokens_ref[...].astype(F32)
    scale = lax.rsqrt(jnp.mean(wide * wide, axis=-1, keepdims=True) + EPS)
    cols = pl.ds(pl.multiple_of(c * half, 128), half)
    part = tokens_ref[:, cols].astype(F32)
    tbuf[pl.ds(g, 1)] = (part * scale * mix_ref[:, cols]).astype(BF16)[None]
    packed[...] = jnp.zeros_like(packed)
    packed[0:6, 0:16] = routes_ref[...].astype(F32)
    packed[8:14, 0:16] = gates_ref[...]
    packed[14:15, 0:16] = lengths_ref[...].astype(F32)
    turned = packed[...].T[0:16]
    earlier = lax.broadcasted_iota(jnp.int32, (16, 16), 1) < lax.broadcasted_iota(
        jnp.int32, (16, 16), 0
    )
    column_of = lax.broadcasted_iota(jnp.int32, (16, 16), 1)
    table = turned
    for k in range(6):
        same = jnp.zeros((16, 16), F32)
        for other in range(6):
            same = jnp.where(
                turned[:, k : k + 1] == packed[other : other + 1, 0:16], 1.0, same
            )
        rank = jnp.max(jnp.where(earlier, same, 0.0), axis=1, keepdims=True)
        table = jnp.where(column_of == k, turned * 2.0 + rank, table)
    rt[:, 0:16] = table
    angles = turned[:, 14:15] * freq_ref[...]
    first = lax.broadcasted_iota(jnp.int32, (16, 128), 1) % 64 < 32
    trig[0] = jnp.cos(angles)
    sines = jnp.sin(angles)
    trig[1] = jnp.where(first, -sines, sines)
    pl.semaphore_wait(barrier, 2 * NG - 1 + 2 * NZ - 2)

    def plane(src, dst, send, recv):
        return Group(g, NG, lambda k: device(z, k, c), src, dst, send, recv)

    def column(src, dst, send, recv):
        return Group(z, NZ, lambda k: device(k, g, c), src, dst, send, recv)

    ga = plane(lambda k: wsrc.at[k], lambda k: abuf.at[k], a_s, a_r)
    gt = plane(lambda k: tbuf.at[g], lambda k: tbuf.at[k], t_s, t_r)
    gc = column(lambda k: wot_ref, lambda k: zbuf.at[k], c_s, c_r)
    gq = column(lambda k: rt, lambda k: qbuf.at[k], q_s, q_r)
    ga.start()
    own_a = pltpu.make_async_copy(wsrc.at[g], abuf.at[g], l_s.at[0])
    own_a.start()
    gc.start()
    gq.start()
    own_z = pltpu.make_async_copy(wot_ref, zbuf.at[z], l_s.at[1])
    own_z.start()
    qbuf[pl.ds(z, 1), :, 0:16] = rt[:, 0:16][None]

    ga.wait()
    own_a.wait()
    b_core = z >> 2

    def b_copy(n, delta):
        return remote(
            abuf,
            wbuf.at[c, z & 3],
            b_s.at[n],
            b_r.at[c, z & 3],
            device((z + delta) & (NZ - 1), g, b_core),
        )

    direct = ((0, 2), (1, -2), (2, 1), (3, -1))
    for n, delta in direct:
        b_copy(n, delta).start()

    @pl.when(b_core == c)
    def _():
        pltpu.make_async_copy(abuf, wbuf.at[c, z & 3], b_r.at[c, z & 3]).start()

    @pl.when(b_core != c)
    def _():
        b_copy(4, 0).start()

    gt.start()

    def onward(delta, to, n, half_of):
        source = (z + delta) & (NZ - 1)
        block = wbuf.at[half_of, source & 3]
        return remote(
            block,
            block,
            n_s.at[half_of, n],
            b_r.at[half_of, source & 3],
            device((z + to) & (NZ - 1), g, c),
        )

    hops = ((-2, ((1, 0), (2, 1))), (2, ((-1, 2),)))

    def forwards(act):
        for delta, targets in hops:

            @pl.when((((z + delta) & (NZ - 1)) >> 2) == c)
            def _(delta=delta, targets=targets):
                for half_of in range(2):
                    act(delta, targets, half_of)

    def pass_on(delta, targets, half_of):
        source = (z + delta) & 3
        pltpu.make_async_copy(
            abuf, wbuf.at[half_of, source], b_r.at[half_of, source]
        ).wait()
        for to, n in targets:
            onward(delta, to, n, half_of).start()

    gc.wait()
    own_z.wait()
    to_half = g >> 3

    def d_copy(k):
        other = 2 * k + to_half
        return other, remote(
            zbuf.at[k], wo.at[(g & 7)], d_s.at[k], d_r.at[(g & 7)], device(z, other, c)
        )

    def d_start(k):
        other, copy = d_copy(k)

        @pl.when(other == g)
        def _():
            pltpu.make_async_copy(zbuf.at[k], wo.at[(g & 7)], d_r.at[(g & 7)]).start()

        @pl.when(other != g)
        def _():
            copy.start()

    each(0, NZ, d_start)
    forwards(pass_on)

    gq.wait()
    routing = qbuf[...].reshape(NZ * 16, 128)
    slots = 16 * NG
    row_z = lax.broadcasted_iota(jnp.int32, (NZ * 16, slots), 0) // 16
    lane = lax.broadcasted_iota(jnp.int32, (NZ * 16, slots), 1)
    slot_id = ((z * NG + lane // 16) * 2 + lane % 2).astype(F32)
    same_z = row_z == (lane % 16) // 2
    named = jnp.zeros((NZ * 16, slots), F32)
    weight = jnp.zeros((NZ * 16, slots), F32)
    for k in range(6):
        hit = jnp.logical_and(routing[:, k : k + 1] == slot_id, same_z)
        named = named + jnp.where(hit, 1.0, 0.0)
        weight = weight + jnp.where(hit, routing[:, 8 + k : 9 + k], 0.0)
    onehot[...] = named.T.astype(BF16)
    upper = weight.astype(BF16)
    comb_hi[...] = upper
    comb_lo[...] = (weight - upper.astype(F32)).astype(BF16)

    gt.wait()

    def b_wait(j):
        source = c * 4 + (j & 3)

        @pl.when(((source - z) & 3) != 2)
        def _():
            pltpu.make_async_copy(abuf, wbuf.at[j >> 2, j & 3], b_r.at[j >> 2, j & 3]).wait()

    each(0, NZ, b_wait)
    rows = NG * tbuf.shape[1]
    normed = tbuf[...].reshape(rows, half)

    def weights(k):
        return wbuf[pl.ds(k, 1)].reshape(half, 128)

    xsend[...] = dot(normed, weights(1 - c))
    swap = remote(xsend, xbuf, x_s.at[0], x_r.at[0], device(z, g, 1 - c))
    swap.start()
    mine = dot(normed, weights(c))
    swap.wait_recv()
    osend[...] = (mine + xbuf[...]).astype(BF16).reshape(osend.shape)
    go = plane(lambda k: osend.at[k], lambda k: obuf.at[k], o_s, o_r)
    go.start()
    obuf[pl.ds(g, 1)] = osend[pl.ds(g, 1)]
    for group in (ga, gt, gc, gq):
        group.drain()
    for n, delta in direct:
        b_copy(n, delta).wait_send()

    @pl.when(b_core != c)
    def _():
        b_copy(4, 0).wait_send()

    def sent_on(delta, targets, half_of):
        for to, n in targets:
            onward(delta, to, n, half_of).wait_send()

    forwards(sent_on)
    swap.wait_send()

    def d_sent(k):
        other, copy = d_copy(k)

        @pl.when(other != g)
        def _():
            copy.wait_send()

    each(0, NZ, d_sent)
    loads[0].wait()
    fs[...] = jnp.zeros_like(fs)
    go.wait()

    low_half = lax.broadcasted_iota(jnp.int32, (16, 128), 1) < 64
    def rotate(v):
        other = jnp.where(first, pltpu.roll(v, 96, 1), pltpu.roll(v, 32, 1))
        return v * trig[0] + other * trig[1]

    def by_head(v):
        low = jnp.sum(jnp.where(low_half, v, 0.0), axis=-1, keepdims=True)
        high = jnp.sum(jnp.where(low_half, 0.0, v), axis=-1, keepdims=True)
        return jnp.where(low_half, low, high)

    def read_pair(hp):
        def block(k):
            return obuf[pl.ds(4 * k + hp, 1)][0].astype(F32)

        query = rotate(block(0))
        key = rotate(block(1)) * HEAD ** (-0.5)
        value = block(2)
        query_t = query.T
        kt[pl.ds(hp, 1)] = key.T[None]
        vsc[pl.ds(2 * hp, 1)] = value[None]
        vsc[pl.ds(2 * hp + 1, 1)] = pltpu.roll(value, 64, 1)[None]
        for h in range(2):
            for s in range(16):
                held = state[s, pl.ds(2 * hp + h, 1)][0]
                column_q = query_t[h * 64 : (h + 1) * 64, s : s + 1]
                fs[h, s : s + 1, 0:64] = jnp.sum(column_q * held, axis=0, keepdims=True)
        from_state = jnp.where(low_half, fs[0], pltpu.roll(fs[1], 64, 1))
        decay = decay_of((c * 8 + 2 * hp + jnp.where(low_half[0:1], 0, 1)).astype(F32))
        read = decay * from_state + by_head(query * key) * value
        read = read * lax.rsqrt(by_head(read * read) / HEAD + EPS)
        rbuf[pl.ds(g, 1), pl.ds(hp, 1)] = (read * jax.nn.silu(block(3))).astype(BF16)[None, None]

    each(0, 4, read_pair)
    gr = plane(lambda k: rbuf.at[g], lambda k: rbuf.at[k], r_s, r_r)
    gr.start()

    def update_pair(hp):
        keys = kt[pl.ds(hp, 1)][0]
        for h in range(2):
            decay = decay_of(jnp.full((1, 64), c * 8 + 2 * hp + h, jnp.int32).astype(F32))
            value = vsc[pl.ds(2 * hp + h, 1)][0]
            for s in range(16):
                held = state[s, pl.ds(2 * hp + h, 1)][0]
                column_k = keys[h * 64 : (h + 1) * 64, s : s + 1]
                state[s, pl.ds(2 * hp + h, 1)] = (
                    decay * held + column_k * value[s : s + 1, 0:64]
                )[None]

    each(0, 4, update_pair)
    def d_wait(k):
        pltpu.make_async_copy(zbuf.at[k], wo.at[k], d_r.at[k]).wait()

    each(0, NZ, d_wait)
    go.drain()
    gr.wait()

    partial = dot(wide_rows(rbuf[...]), wo[...].reshape(128, 512), ((1,), (1,)))
    psend[...] = partial.astype(BF16).reshape(psend.shape)
    gp = [
        plane(lambda k: psend.at[k], lambda k: pbuf.at[c, k], p_s.at[0], p_r.at[c]),
    ]
    gp[0].start()
    gp_other = Group(
        g, NG, lambda k: device(z, k, 1 - c), lambda k: psend.at[k], lambda k: pbuf.at[c, k],
        p_s.at[1], p_r.at[c],
    )
    each(0, NG, lambda i: gp_other.out(i).start())
    pbuf[pl.ds(c, 1), pl.ds(g, 1)] = psend[pl.ds(g, 1)][None]
    gr.drain()
    gp[0].wait()
    gp_from = Group(
        g, NG, lambda k: device(z, k, 1 - c), lambda k: psend.at[k], lambda k: pbuf.at[1 - c, k],
        p_s.at[1], p_r.at[1 - c],
    )
    each(0, NG, lambda i: gp_from.come(i).wait_recv())
    mixed = (pbuf[0].astype(F32) + pbuf[1].astype(F32)).astype(BF16).astype(F32)
    tok = jnp.stack([tokens_ref[:, k * 128 : (k + 1) * 128] for k in range(NG)]).astype(F32)
    mid = (tok + mixed * row_scale(mixed) * post_ref[...]).astype(BF16)
    middle[...] = mid
    mid = mid.astype(F32)
    mo[...] = (mid * row_scale(mid) * ffn_ref[...]).astype(BF16)

    own_blocks = pl.ds(pl.multiple_of(c * 8, 8), 8)
    mbuf[pl.ds(z, 1)] = mo[own_blocks][None]
    gm = column(lambda k: mbuf.at[z], lambda k: mbuf.at[k], m_s, m_r)
    gm.start()
    for load in loads[1:4]:
        load.wait()
    rows_in = wide_rows(mo[...][None])
    shared_hidden = (jax.nn.silu(dot(rows_in, sg[...])) * dot(rows_in, su[...])).astype(BF16)
    shared_part = dot(shared_hidden, sd[...]).astype(BF16)
    parts = jnp.stack([shared_part[:, k * 128 : (k + 1) * 128] for k in range(NG)])
    shs[...] = parts.reshape(shs.shape)
    share = remote(shs.at[1 - c], shb, x_s.at[1], x_r.at[1], device(z, g, 1 - c))
    share.start()
    gp[0].drain()
    each(0, NG, lambda i: gp_other.out(i).wait_send())
    for load in loads[4:]:
        load.wait()
    gm.wait()
    sorted_rows = dot(onehot[...], wide_rows(mbuf[...])).astype(BF16)
    for k in range(8):
        ysend[:, k] = sorted_rows[:, k * 128 : (k + 1) * 128].reshape(NG, 16, 128)
    gy = plane(lambda k: ysend.at[k], lambda k: ebuf.at[c, k], y_s, y_r)
    gy.start()
    ebuf[pl.ds(c, 1), pl.ds(g, 1)] = ysend[pl.ds(g, 1)][None]

    def forward(half_from, k):
        return remote(
            ebuf.at[half_from, k], ebuf.at[half_from, k], f_s.at[k], f_r.at[k], device(z, g, 1 - c)
        )

    forward(c, g).start()

    def relay(i):
        gy.come(i).wait_recv()
        forward(c, (g + i) & (NG - 1)).start()

    gm.drain()
    each(1, NG, relay)

    def expert_in(k):
        blocks = wide_rows(ebuf[pl.ds(k, 1)][0])
        rows_of = pl.ds(pl.multiple_of(k * half, 128), half)
        return dot(blocks, eg[0, rows_of]), dot(blocks, eu[0, rows_of])

    gate_c, up_c = expert_in(c)
    each(0, NG, lambda k: forward(1 - c, k).wait_recv())
    gate_o, up_o = expert_in(1 - c)
    hidden = (jax.nn.silu(gate_c + gate_o) * (up_c + up_o)).astype(BF16)

    def down(k):
        out = dot(hidden, ed[0, :, pl.ds(pl.multiple_of(k * half, 128), half)]).astype(BF16)
        return [out[:, j * 128 : (j + 1) * 128].reshape(NG, 16, 128) for j in range(8)]

    for j, block in enumerate(down(1 - c)):
        dsend[:, j] = block
    give = remote(dsend, dbuf, x_s.at[2], x_r.at[2], device(z, g, 1 - c))
    give.start()
    kept = down(c)
    give.wait_recv()
    for j in range(8):
        ret[:, j] = (kept[j].astype(F32) + dbuf[:, j].astype(F32)).astype(BF16)
    gg = plane(lambda k: ret.at[k], lambda k: back.at[k], g_s, g_r)
    gg.start()
    back[pl.ds(g, 1)] = ret[pl.ds(g, 1)]
    share.wait_recv()
    shared_out = (shs[pl.ds(c, 1)][0].astype(F32) + shb[...].astype(F32)).astype(BF16).astype(F32)
    gy.drain()
    each(0, NG, lambda k: forward(c, k).wait_send())
    share.wait_send()
    give.wait_send()
    gg.wait()

    answers = wide_rows(back[...])
    sums = (dot(comb_hi[...], answers) + dot(comb_lo[...], answers)).astype(BF16)
    for k in range(8):
        csend[:, k] = sums[:, k * 128 : (k + 1) * 128].reshape(NZ, 16, 128)
    gh = column(lambda k: csend.at[k], lambda k: cbuf.at[k], h_s, h_r)
    gh.start()
    cbuf[pl.ds(z, 1)] = csend[pl.ds(z, 1)]
    gg.drain()
    gh.wait()
    mixs[...] = shared_out + jnp.sum(cbuf[...].astype(F32), axis=0)
    last = remote(mixs, mixb, x_s.at[3], x_r.at[3], device(z, g, 1 - c))
    last.start()
    last.wait_recv()
    first_half = jnp.where(c == 0, mixs[...], mixb[...])
    second_half = jnp.where(c == 0, mixb[...], mixs[...])
    mixture = jnp.concatenate([first_half, second_half], axis=0)
    final = (middle[...].astype(F32) + mixture * row_scale(mixture) * outg_ref[...]).astype(BF16)
    for k in range(NG):
        result_ref[:, k * 128 : (k + 1) * 128] = final[k]

    gh.drain()
    last.wait_send()


def on_device(
    tokens, lengths, prior_state, mix_gain, post_gain, ffn_gain, out_gain,
    query_weight, key_weight, value_weight, gate_weight, out_weight, routes, route_gates,
    expert_gate, expert_up, expert_down, shared_gate, shared_up, shared_down,
):
    seq, width = tokens.shape
    frequency = THETA ** (-(np.arange(128) % 32).astype(np.float64) / 32)
    dma = pltpu.SemaphoreType.DMA
    blocks = pltpu.VMEM((NG, 16, 128), BF16)
    halves = pltpu.VMEM((NG, 8, 16, 128), BF16)
    square = pltpu.VMEM((NG * seq, 128), F32)
    vmem = pl.BlockSpec(memory_space=pltpu.VMEM)
    anywhere = pl.BlockSpec(memory_space=pl.ANY)
    big = (prior_state, expert_gate, expert_up, expert_down, shared_gate, shared_up, shared_down)
    plane_sems, column_sems = dma((NG,)), dma((NZ,))
    return pl.pallas_call(
        layer_kernel,
        out_shape=(
            pltpu.VMEM((seq, width), BF16),
            pltpu.VMEM(prior_state.shape, F32),
        ),
        in_specs=[vmem] * 14 + [anywhere] * 7,
        out_specs=(vmem, vmem),
        scratch_shapes=[
            *(pltpu.VMEM(array.shape, array.dtype) for array in big[1:]),
            blocks,
            pltpu.VMEM((16, 128), F32),
            pltpu.VMEM((16, 128), F32),
            pltpu.VMEM((2, 16, 128), F32),
            pltpu.VMEM((NG, seq, width // 2), BF16),
            blocks,
            pltpu.VMEM((2, 4, NG, 16, 128), BF16),
            pltpu.VMEM((8, 16, 512), BF16),
            pltpu.VMEM((8, 16, 512), BF16),
            square,
            square,
            blocks,
            blocks,
            pltpu.VMEM((NZ, 16, 128), F32),
            pltpu.VMEM((16 * NG, 16 * NZ), BF16),
            pltpu.VMEM((16 * NZ, 16 * NG), BF16),
            pltpu.VMEM((16 * NZ, 16 * NG), BF16),
            pltpu.VMEM((4, 128, 16), F32),
            pltpu.VMEM((8, 16, 128), F32),
            pltpu.VMEM((2, 16, 128), F32),
            pltpu.VMEM((NG, 4, 16, 128), BF16),
            blocks,
            pltpu.VMEM((2, NG, 16, 128), BF16),
            blocks,
            blocks,
            pltpu.VMEM((NZ, 8, 16, 128), BF16),
            pltpu.VMEM((2, 8, 16, 128), BF16),
            pltpu.VMEM((8, 16, 128), BF16),
            halves,
            pltpu.VMEM((2, NG, 8, 16, 128), BF16),
            halves,
            halves,
            halves,
            halves,
            pltpu.VMEM((NZ, 8, 16, 128), BF16),
            pltpu.VMEM((NZ, 8, 16, 128), BF16),
            pltpu.VMEM((8, 16, 128), F32),
            pltpu.VMEM((8, 16, 128), F32),
            dma((2,)),
            dma((8,)),
            plane_sems, plane_sems,
            plane_sems, plane_sems,
            dma((5,)), dma((2, 3)), dma((2, 4)),
            column_sems, column_sems,
            column_sems, column_sems,
            column_sems, column_sems,
            plane_sems, plane_sems,
            plane_sems, plane_sems,
            dma((2, NG)), dma((2, NG)),
            column_sems, column_sems,
            plane_sems, plane_sems,
            plane_sems, plane_sems,
            plane_sems, plane_sems,
            column_sems, column_sems,
            dma((4,)), dma((4,)),
        ],
        compiler_params=pltpu.CompilerParams(
            collective_id=0, has_side_effects=True, vmem_limit_bytes=int(59.5 * 2**20)
        ),
        name="layer",
    )(
        tokens,
        lengths[None],
        mix_gain[None],
        *(gain.reshape(NG, 1, 128) for gain in (post_gain, ffn_gain, out_gain)),
        query_weight,
        key_weight,
        value_weight,
        gate_weight,
        out_weight.T,
        routes.T,
        route_gates.T,
        jnp.asarray(frequency[None], F32),
        *big,
    )


def solution(mesh):
    finer = Mesh(mesh.devices.reshape(8, 4, 4, mesh.shape["tp"]), ("ep_0", "ep_1", "ep_2", "tp"))
    in_specs = (
        P(EP, None),
        P(EP),
        P(EP, "tp", None, None),
        P(),
        P(),
        P(),
        P(),
        P(EP, "tp"),
        P(EP, "tp"),
        P(EP, "tp"),
        P(EP, "tp"),
        P("tp", EP),
        P(EP, None),
        P(EP, None),
        P(EP, None, "tp"),
        P(EP, None, "tp"),
        P(EP, "tp", None),
        P(None, "tp"),
        P(None, "tp"),
        P("tp", None),
    )
    out_specs = (P(EP, None), P(EP, "tp", None, None))
    return jax.shard_map(
        on_device, mesh=finer, in_specs=in_specs, out_specs=out_specs, check_vma=False
    )
```

```python
import jax
import jax.numpy as jnp
import numpy as np
from jax import lax
from jax.experimental import pallas as pl
from jax.experimental.pallas import tpu as pltpu
from jax.sharding import Mesh
from jax.sharding import PartitionSpec as P

HEAD = 64
HEADS = 16
EP = ("ep_0", "ep_1", "ep_2")
EPS = 1e-06
THETA = 10000.0
MESH = pl.DeviceIdType.MESH
NZ, NY, NX, NG = 8, 4, 4, 16
NCH = 4
PER = 8 // NCH
BF16 = jnp.bfloat16
F32 = jnp.float32


def place():
    z, y, x, c = (lax.axis_index(name) for name in ("ep_0", "ep_1", "ep_2", "tp"))
    return z, y * NX + x, c


def device(z, g, c):
    return (z, g >> 2, g & 3, c)


def remote(src, dst, send_sem, recv_sem, target):
    return pltpu.make_async_remote_copy(
        src_ref=src,
        dst_ref=dst,
        send_sem=send_sem,
        recv_sem=recv_sem,
        device_id=target,
        device_id_type=MESH,
    )


def each(low, high, body):
    def step(i, carry):
        body(i)
        return carry

    lax.fori_loop(low, high, step, 0)


def dot(a, b, dims=((1,), (0,))):
    return lax.dot_general(a, b, (dims, ((), ())), preferred_element_type=F32)


def wide_rows(blocks):
    rows = blocks.shape[0] * blocks.shape[2]
    return jnp.concatenate(
        [blocks[:, k].reshape(rows, 128) for k in range(blocks.shape[1])], axis=1
    )


def row_scale(blocks):
    count = blocks.shape[0] * blocks.shape[2]
    total = jnp.sum(jnp.sum(blocks * blocks, axis=0), axis=-1, keepdims=True)
    return lax.rsqrt(total / count + EPS)[None]


def arrived(blocks, sem):
    pltpu.make_async_copy(blocks, blocks, sem).wait()


class Exchange:
    def __init__(self, me, size, at, src, dst, send, recv):
        self.me, self.size, self.at, self.src, self.dst = me, size, at, src, dst
        self.send, self.recv = send, recv

    def out(self, i):
        k = (self.me + i) & (self.size - 1)
        return remote(self.src(k), self.dst(self.me), self.send, self.recv, self.at(k))

    def start(self, first=1):
        each(first, self.size, lambda i: self.out(i).start())


def layer_kernel(
    tokens_hbm, routes_hbm, gates_hbm, lengths_hbm, freq_hbm, mix_hbm, wot_hbm, post_hbm, ffn_hbm, outg_hbm,
    wq_hbm, wk_hbm, wv_hbm, wg_hbm,
    state_hbm, eg_hbm, eu_hbm, ed_hbm, sg_hbm, su_hbm, sd_hbm,
    result_ref, new_hbm,
    state,
    tokens_ref, routes_ref, gates_ref, lengths_ref, freq_ref, mix_ref, wot_ref, post_ref, ffn_ref, outg_ref,
    eg, eu, ed, sg, su, sd,
    wsrc, packed, rt, trig,
    tbuf, abuf, wbuf, zbuf, wo, osend, obuf, qbuf, onehot, comb_hi, comb_lo,
    qt, kt, vsc, fs, decays, rbuf, psend, pbuf, middle, mo, mbuf, shs, shb, ysend, ebuf, dsend, dbuf, ret, back,
    csend, cbuf, mixs, mixb,
    i_s, v_s, w_s, a_s, a_r, t_s, t_r, u_s, u_r, b_s, n_s, b_r, c_s, c_r, d_s, d_r, q_s, q_r,
    o_s, o_r, r_s, r_r, p_s, p_r, m_s, m_r, y_s, y_r, f_s, f_r, e_s, e_r, g_s, g_r, h_s, h_r, x_s, x_r,
):
    z, g, c = place()
    loads = [
        pltpu.make_async_copy(src, dst, w_s.at[i])
        for i, (src, dst) in enumerate(
            ((state_hbm, state), (sg_hbm, sg), (su_hbm, su), (sd_hbm, sd),
             (eg_hbm, eg), (eu_hbm, eu), (ed_hbm, ed))
        )
    ]
    barrier = pltpu.get_barrier_semaphore()

    for i in range(1, 2 * NG):
        other = (g * 2 + c + i) & (2 * NG - 1)
        pl.semaphore_signal(
            barrier, inc=1, device_id=device(z, other >> 1, other & 1), device_id_type=MESH
        )
    for i in range(1, NZ):
        for core in range(2):
            pl.semaphore_signal(
                barrier, inc=1, device_id=device((z + i) & (NZ - 1), g, core), device_id_type=MESH
            )
    small = [
        pltpu.make_async_copy(src, dst, i_s.at[i])
        for i, (src, dst) in enumerate(
            ((tokens_hbm, tokens_ref), (mix_hbm, mix_ref), (routes_hbm, routes_ref),
             (gates_hbm, gates_ref), (lengths_hbm, lengths_ref), (freq_hbm, freq_ref),
             (wot_hbm, wot_ref), (post_hbm, post_ref), (ffn_hbm, ffn_ref), (outg_hbm, outg_ref))
        )
    ]
    slices = [
        pltpu.make_async_copy(
            w_ref.at[:, pl.ds(k * 128, 128)], wsrc.at[4 * m + k], v_s
        )
        for m, w_ref in enumerate((wq_hbm, wk_hbm, wv_hbm, wg_hbm))
        for k in range(4)
    ]
    for load in small[:2] + slices + small[2:] + loads:
        load.start()
    for load in small[:6]:
        load.wait()
    half = tbuf.shape[-1]
    wide = tokens_ref[...].astype(F32)
    scale = lax.rsqrt(jnp.mean(wide * wide, axis=-1, keepdims=True) + EPS)
    normed = (wide * scale * mix_ref[...]).astype(BF16)
    for k in range(2):
        tbuf[k, pl.ds(g, 1)] = normed[:, k * half : (k + 1) * half][None]
    packed[...] = jnp.zeros_like(packed)
    packed[0:6, 0:16] = routes_ref[...].astype(F32)
    packed[8:14, 0:16] = gates_ref[...]
    packed[14:15, 0:16] = lengths_ref[...].astype(F32)
    turned = packed[...].T[0:16]
    earlier = lax.broadcasted_iota(jnp.int32, (16, 16), 1) < lax.broadcasted_iota(
        jnp.int32, (16, 16), 0
    )
    column_of = lax.broadcasted_iota(jnp.int32, (16, 16), 1)
    table = turned
    for k in range(6):
        same = jnp.zeros((16, 16), F32)
        for other in range(6):
            same = jnp.where(
                turned[:, k : k + 1] == packed[other : other + 1, 0:16], 1.0, same
            )
        rank = jnp.max(jnp.where(earlier, same, 0.0), axis=1, keepdims=True)
        table = jnp.where(column_of == k, turned * 2.0 + rank, table)
    rt[:, 0:16] = table
    for load in small[6:]:
        load.wait()
    arrived(wsrc, v_s)
    pl.semaphore_wait(barrier, 2 * NG - 1 + 2 * NZ - 2)

    def plane(src, dst, send, recv):
        return Exchange(g, NG, lambda k: device(z, k, c), src, dst, send, recv)

    def column(src, dst, send, recv):
        return Exchange(z, NZ, lambda k: device(k, g, c), src, dst, send, recv)

    others, above = pl.ds(0, NG - 1), pl.ds(0, NZ - 1)

    ga = plane(lambda k: wsrc.at[k], lambda k: abuf.at[k], a_s, a_r)
    gt = plane(lambda k: tbuf.at[c, g], lambda k: tbuf.at[c, k], t_s, t_r.at[g])
    gc = column(lambda k: wot_ref, lambda k: zbuf.at[k], c_s, c_r)
    gq = column(lambda k: rt, lambda k: qbuf.at[k], q_s, q_r)
    ga.start()
    pltpu.make_async_copy(wsrc.at[g], abuf.at[g], a_r).start()
    gq.start()
    qbuf[pl.ds(z, 1), :, 0:16] = rt[:, 0:16][None]

    arrived(abuf, a_r)

    def b_copy(delta):
        return remote(
            abuf, wbuf.at[z], b_s, b_r.at[z], device((z + delta) & (NZ - 1), g, c)
        )

    for delta in (2, -2, 1, -1):
        b_copy(delta).start()
    pltpu.make_async_copy(abuf, wbuf.at[z], b_r.at[z]).start()
    gt.start()

    def b_wait(delta):
        source = (z + delta) & (NZ - 1)
        pltpu.make_async_copy(abuf, wbuf.at[source], b_r.at[source]).wait()

    def onward(delta, to):
        source = (z + delta) & (NZ - 1)
        return remote(
            wbuf.at[source],
            wbuf.at[source],
            n_s,
            b_r.at[source],
            device((z + to) & (NZ - 1), g, c),
        )

    to_half = g >> 3

    def d_start(k):
        other = 2 * k + to_half

        @pl.when(other == g)
        def _():
            pltpu.make_async_copy(zbuf.at[k], wo.at[g & 7], d_r).start()

        @pl.when(other != g)
        def _():
            remote(zbuf.at[k], wo.at[g & 7], d_s, d_r, device(z, other, c)).start()

    arrived(qbuf.at[above], q_r)
    routing = qbuf[...].reshape(NZ * 16, 128)
    slots = 16 * NG
    row_z = lax.broadcasted_iota(jnp.int32, (NZ * 16, slots), 0) // 16
    lane = lax.broadcasted_iota(jnp.int32, (NZ * 16, slots), 1)
    slot_id = ((z * NG + lane // 16) * 2 + lane % 2).astype(F32)
    same_z = row_z == (lane % 16) // 2
    named = jnp.zeros((NZ * 16, slots), F32)
    weight = jnp.zeros((NZ * 16, slots), F32)
    for k in range(6):
        hit = jnp.logical_and(routing[:, k : k + 1] == slot_id, same_z)
        named = named + jnp.where(hit, 1.0, 0.0)
        weight = weight + jnp.where(hit, routing[:, 8 + k : 9 + k], 0.0)
    onehot[...] = named.T.astype(BF16)
    upper = weight.astype(BF16)
    comb_hi[...] = upper
    comb_lo[...] = (weight - upper.astype(F32)).astype(BF16)

    angles = rt[:, 14:15] * freq_ref[...]
    first = lax.broadcasted_iota(jnp.int32, (16, 128), 1) % 64 < 32
    trig[0] = jnp.cos(angles)
    sines = jnp.sin(angles)
    trig[1] = jnp.where(first, -sines, sines)
    heads = lax.broadcasted_iota(jnp.int32, (8, 128), 0) + c * 8
    decays[...] = 1.0 - jnp.exp2(-5.0 - 7.0 * heads.astype(F32) / (HEADS - 1))
    b_wait(-2)
    onward(-2, 2).start()
    onward(-2, 1).start()
    b_wait(2)
    onward(2, -1).start()

    def t_forward(half_of, k):
        block = tbuf.at[half_of, k]
        return remote(block, block, u_s, u_r, device(z, g, 1 - c))

    def t_relay(i):
        k = (g + i) & (NG - 1)
        arrived(tbuf.at[c, k], t_r.at[k])
        t_forward(c, k).start()

    each(1, NG, t_relay)
    arrived(tbuf.at[1 - c, others], u_r)

    for delta in (0, 1, -1, 3, -3, 4):
        b_wait(delta)
    rows = NG * tbuf.shape[2]
    mine = dot(tbuf[0].reshape(rows, half), wbuf[0:4].reshape(half, 128)) + dot(
        tbuf[1].reshape(rows, half), wbuf[4:8].reshape(half, 128)
    )
    osend[...] = mine.astype(BF16).reshape(osend.shape)
    go = plane(lambda k: osend.at[k], lambda k: obuf.at[k], o_s, o_r)
    go.start()
    gc = column(lambda k: wot_ref, lambda k: zbuf.at[z], c_s, c_r)
    gc.start()
    pltpu.make_async_copy(wot_ref, zbuf.at[z], c_r).start()
    obuf[pl.ds(g, 1)] = osend[pl.ds(g, 1)]
    arrived(abuf.at[others], a_s)
    arrived(tbuf.at[c, others], t_s)
    arrived(tbuf.at[c, others], u_s)
    arrived(qbuf.at[above], q_s)
    arrived(wbuf.at[pl.ds(0, 4)], b_s)
    arrived(wbuf.at[pl.ds(0, 3)], n_s)
    loads[0].wait()
    arrived(obuf.at[others], o_r)
    arrived(zbuf, c_r)
    each(0, NZ, d_start)
    low_half = lax.broadcasted_iota(jnp.int32, (16, 128), 1) < 64
    def rotate(v):
        other = jnp.where(first, pltpu.roll(v, 96, 1), pltpu.roll(v, 32, 1))
        return v * trig[0] + other * trig[1]

    def by_head(v):
        low = jnp.sum(jnp.where(low_half, v, 0.0), axis=-1, keepdims=True)
        high = jnp.sum(jnp.where(low_half, 0.0, v), axis=-1, keepdims=True)
        return jnp.where(low_half, low, high)

    def block(k, hp):
        return obuf[4 * k + hp].astype(F32)

    self_terms = []
    for hp in range(4):
        query = rotate(block(0, hp))
        key = rotate(block(1, hp)) * HEAD ** (-0.5)
        value = block(2, hp)
        qt[hp] = query.T
        kt[hp] = key.T
        vsc[2 * hp] = value
        vsc[2 * hp + 1] = pltpu.roll(value, 64, 1)
        self_terms.append(by_head(query * key) * value)

    def read_pair(hp):
        queries = qt[pl.ds(hp, 1)][0]
        for h in range(2):
            for s in range(16):
                held = state[s, pl.ds(2 * hp + h, 1)][0]
                column_q = queries[h * 64 : (h + 1) * 64, s : s + 1]
                fs[pl.ds(2 * hp + h, 1), s : s + 1, 0:64] = jnp.sum(
                    column_q * held, axis=0, keepdims=True
                )[None]

    each(0, 4, read_pair)
    for hp in range(4):
        from_state = jnp.where(low_half, fs[2 * hp], pltpu.roll(fs[2 * hp + 1], 64, 1))
        decay = jnp.where(
            low_half[0:1], decays[2 * hp : 2 * hp + 1], decays[2 * hp + 1 : 2 * hp + 2]
        )
        read = decay * from_state + self_terms[hp]
        read = read * lax.rsqrt(by_head(read * read) / HEAD + EPS)
        rbuf[pl.ds(g, 1), hp] = (read * jax.nn.silu(block(3, hp))).astype(BF16)[None]
    gr = plane(lambda k: rbuf.at[g], lambda k: rbuf.at[g], r_s, r_r)
    gr.start()

    def update_pair(hp):
        keys = kt[pl.ds(hp, 1)][0]
        for h in range(2):
            decay = decays[pl.ds(2 * hp + h, 1), 0:64]
            value = vsc[pl.ds(2 * hp + h, 1)][0]
            for s in range(16):
                held = state[s, pl.ds(2 * hp + h, 1)][0]
                column_k = keys[h * 64 : (h + 1) * 64, s : s + 1]
                state[s, pl.ds(2 * hp + h, 1)] = (
                    decay * held + column_k * value[s : s + 1, 0:64]
                )[None]

    each(0, 4, update_pair)
    def d_wait(k):
        pltpu.make_async_copy(zbuf.at[k], wo.at[k], d_r.at[k]).wait()

    store = pltpu.make_async_copy(state, new_hbm, w_s.at[7])
    store.start()
    arrived(obuf.at[others], o_s)
    arrived(zbuf.at[above], c_s)

    @pl.when((g & 1) == to_half)
    def _():
        arrived(zbuf.at[above], d_s)

    @pl.when((g & 1) != to_half)
    def _():
        arrived(zbuf, d_s)

    arrived(wo, d_r)
    arrived(rbuf.at[others], r_r)
    partial = dot(wide_rows(rbuf[...]), wo[...].reshape(128, 512), ((1,), (1,)))
    psend[...] = partial.astype(BF16).reshape(psend.shape)
    gp = plane(lambda k: psend.at[k], lambda k: pbuf.at[c, k], p_s.at[0], p_r.at[0])
    gp.start()
    gp_other = Exchange(
        g, NG, lambda k: device(z, k, 1 - c), lambda k: psend.at[k], lambda k: pbuf.at[c, k],
        p_s.at[1], p_r.at[1],
    )
    gp_other.start(0)
    pbuf[pl.ds(c, 1), pl.ds(g, 1)] = psend[pl.ds(g, 1)][None]
    arrived(rbuf.at[others], r_s)
    arrived(psend.at[others], p_r.at[0])
    arrived(psend, p_r.at[1])
    mixed = (pbuf[0].astype(F32) + pbuf[1].astype(F32)).astype(BF16).astype(F32)
    tok = jnp.stack([tokens_ref[:, k * 128 : (k + 1) * 128] for k in range(NG)]).astype(F32)
    mid = (tok + mixed * row_scale(mixed) * post_ref[...]).astype(BF16)
    middle[...] = mid
    mid = mid.astype(F32)
    mo[...] = (mid * row_scale(mid) * ffn_ref[...]).astype(BF16)

    for n in range(NCH):
        blocks = pl.ds(c * 8 + n * PER, PER)
        mbuf[n, pl.ds(z, 1)] = mo[blocks][None]
        gm = column(lambda k, n=n: mbuf.at[n, z], lambda k, n=n: mbuf.at[n, k], m_s, m_r.at[n])
        gm.start()
    for load in loads[1:4]:
        load.wait()
    rows_in = wide_rows(mo[...][None])
    shared_hidden = (jax.nn.silu(dot(rows_in, sg[...])) * dot(rows_in, su[...])).astype(BF16)
    shared_part = dot(shared_hidden, sd[...]).astype(BF16)
    parts = jnp.stack([shared_part[:, k * 128 : (k + 1) * 128] for k in range(NG)])
    shs[...] = parts.reshape(shs.shape)
    share = remote(shs.at[1 - c], shb, x_s.at[0], x_r.at[0], device(z, g, 1 - c))
    share.start()
    for load in loads[4:]:
        load.wait()
    arrived(psend.at[others], p_s.at[0])
    arrived(psend, p_s.at[1])
    for n in range(NCH):
        arrived(mbuf.at[n, above], m_r.at[n])
        sorted_rows = dot(onehot[...], wide_rows(mbuf[n])).astype(BF16)
        for k in range(PER):
            ysend[n, :, k] = sorted_rows[:, k * 128 : (k + 1) * 128].reshape(NG, 16, 128)
        gy = plane(lambda k, n=n: ysend.at[n, k], lambda k, n=n: ebuf.at[n, c, k], y_s, y_r.at[n])
        gy.start()
        ebuf[n, pl.ds(c, 1), pl.ds(g, 1)] = ysend[n, pl.ds(g, 1)][None]
    arrived(mbuf.at[:, above], m_s)

    def forward(n):
        rows = ebuf.at[n, c]
        return remote(rows, rows, f_s.at[n], f_r.at[n], device(z, g, 1 - c))

    def expert_in(n, k):
        blocks = wide_rows(ebuf[n, pl.ds(k, 1)][0])
        rows_of = pl.ds(pl.multiple_of(k * half + n * PER * 128, 128), PER * 128)
        return dot(blocks, eg[0, rows_of]), dot(blocks, eu[0, rows_of])

    gates, ups = [], []
    for n in range(NCH):
        arrived(ebuf.at[n, c, others], y_r.at[n])
        forward(n).start()
        gate, up = expert_in(n, c)
        gates.append(gate)
        ups.append(up)
    for n in range(NCH):
        arrived(ebuf.at[n, 1 - c], f_r.at[n])
        gate, up = expert_in(n, 1 - c)
        gates.append(gate)
        ups.append(up)
    hidden = (jax.nn.silu(sum(gates)) * sum(ups)).astype(BF16)

    def down(n, k):
        cols_of = pl.ds(pl.multiple_of(k * half + n * PER * 128, 128), PER * 128)
        out = dot(hidden, ed[0, :, cols_of]).astype(BF16)
        return [out[:, j * 128 : (j + 1) * 128].reshape(NG, 16, 128) for j in range(PER)]

    def give(n):
        return remote(dsend.at[n], dbuf.at[n], e_s.at[n], e_r.at[n], device(z, g, 1 - c))

    for n in range(NCH):
        for j, rows in enumerate(down(n, 1 - c)):
            dsend[n, :, j] = rows
        give(n).start()
    for n in range(NCH):
        kept = down(n, c)
        give(n).wait_recv()
        for j in range(PER):
            ret[n, :, j] = (kept[j].astype(F32) + dbuf[n, :, j].astype(F32)).astype(BF16)
        gg = plane(lambda k, n=n: ret.at[n, k], lambda k, n=n: back.at[n, k], g_s, g_r.at[n])
        gg.start()
        back[n, pl.ds(g, 1)] = ret[n, pl.ds(g, 1)]
    share.wait_recv()
    shared_out = (shs[pl.ds(c, 1)][0].astype(F32) + shb[...].astype(F32)).astype(BF16).astype(F32)
    arrived(ysend.at[:, others], y_s)
    for n in range(NCH):
        forward(n).wait_send()
        give(n).wait_send()
    share.wait_send()

    for n in range(NCH):
        arrived(back.at[n, others], g_r.at[n])
        answers = wide_rows(back[n])
        sums = (dot(comb_hi[...], answers) + dot(comb_lo[...], answers)).astype(BF16)
        for k in range(PER):
            csend[n, :, k] = sums[:, k * 128 : (k + 1) * 128].reshape(NZ, 16, 128)
        gh = column(lambda k, n=n: csend.at[n, k], lambda k, n=n: cbuf.at[n, k], h_s, h_r.at[n])
        gh.start()
        cbuf[n, pl.ds(z, 1)] = csend[n, pl.ds(z, 1)]
    arrived(ret.at[:, others], g_s)
    for n in range(NCH):
        arrived(cbuf.at[n, above], h_r.at[n])
        part = slice(n * PER, (n + 1) * PER)
        mixs[part] = shared_out[part] + jnp.sum(cbuf[n].astype(F32), axis=0)
    last = remote(mixs, mixb, x_s.at[1], x_r.at[1], device(z, g, 1 - c))
    last.start()
    last.wait_recv()
    first_half = jnp.where(c == 0, mixs[...], mixb[...])
    second_half = jnp.where(c == 0, mixb[...], mixs[...])
    mixture = jnp.concatenate([first_half, second_half], axis=0)
    final = (middle[...].astype(F32) + mixture * row_scale(mixture) * outg_ref[...]).astype(BF16)
    for k in range(NG):
        result_ref[:, k * 128 : (k + 1) * 128] = final[k]
    arrived(csend.at[:, above], h_s)
    last.wait_send()
    store.wait()


def on_device(
    tokens, lengths, prior_state, mix_gain, post_gain, ffn_gain, out_gain,
    query_weight, key_weight, value_weight, gate_weight, out_weight, routes, route_gates,
    expert_gate, expert_up, expert_down, shared_gate, shared_up, shared_down,
):
    seq, width = tokens.shape
    frequency = THETA ** (-(np.arange(128) % 32).astype(np.float64) / 32)
    dma = pltpu.SemaphoreType.DMA
    blocks = pltpu.VMEM((NG, 16, 128), BF16)
    halves = pltpu.VMEM((NCH, NG, PER, 16, 128), BF16)
    columns_of = pltpu.VMEM((NCH, NZ, PER, 16, 128), BF16)
    vmem = pl.BlockSpec(memory_space=pltpu.VMEM)
    anywhere = pl.BlockSpec(memory_space=pl.ANY)
    big = (prior_state, expert_gate, expert_up, expert_down, shared_gate, shared_up, shared_down)
    chunk_sems = dma((NCH,))
    post, ffn, outer = (gain.reshape(NG, 1, 128) for gain in (post_gain, ffn_gain, out_gain))
    small = (
        tokens, routes.T, route_gates.T, lengths[None], jnp.asarray(frequency[None], F32),
        mix_gain[None], out_weight.T, post, ffn, outer,
    )
    columns = (query_weight, key_weight, value_weight, gate_weight)
    return pl.pallas_call(
        layer_kernel,
        out_shape=(
            pltpu.VMEM((seq, width), BF16),
            pltpu.VMEM(prior_state.shape, F32),
        ),
        in_specs=[anywhere] * (len(small) + len(columns) + len(big)),
        out_specs=(vmem, anywhere),
        scratch_shapes=[
            pltpu.VMEM(prior_state.shape, F32),
            *(pltpu.VMEM(array.shape, array.dtype) for array in small + big[1:]),
            blocks,
            pltpu.VMEM((16, 128), F32),
            pltpu.VMEM((16, 128), F32),
            pltpu.VMEM((2, 16, 128), F32),
            pltpu.VMEM((2, NG, seq, width // 2), BF16),
            blocks,
            pltpu.VMEM((NZ, NG, 16, 128), BF16),
            pltpu.VMEM((8, 16, 512), BF16),
            pltpu.VMEM((8, 16, 512), BF16),
            blocks,
            blocks,
            pltpu.VMEM((NZ, 16, 128), F32),
            pltpu.VMEM((16 * NG, 16 * NZ), BF16),
            pltpu.VMEM((16 * NZ, 16 * NG), BF16),
            pltpu.VMEM((16 * NZ, 16 * NG), BF16),
            pltpu.VMEM((4, 128, 16), F32),
            pltpu.VMEM((4, 128, 16), F32),
            pltpu.VMEM((8, 16, 128), F32),
            pltpu.VMEM((8, 16, 128), F32),
            pltpu.VMEM((8, 128), F32),
            pltpu.VMEM((NG, 4, 16, 128), BF16),
            blocks,
            pltpu.VMEM((2, NG, 16, 128), BF16),
            blocks,
            blocks,
            columns_of,
            pltpu.VMEM((2, 8, 16, 128), BF16),
            pltpu.VMEM((8, 16, 128), BF16),
            halves,
            pltpu.VMEM((NCH, 2, NG, PER, 16, 128), BF16),
            halves,
            halves,
            halves,
            halves,
            columns_of,
            columns_of,
            pltpu.VMEM((8, 16, 128), F32),
            pltpu.VMEM((8, 16, 128), F32),
            dma((len(small),)),
            dma,
            dma((8,)),
            dma, dma,
            dma, dma((NG,)),
            dma, dma,
            dma, dma, dma((NZ,)),
            dma, dma, dma, dma, dma, dma,
            dma, dma, dma, dma,
            dma((2,)), dma((2,)),
            dma, chunk_sems,
            dma, chunk_sems,
            chunk_sems, chunk_sems,
            chunk_sems, chunk_sems,
            dma, chunk_sems,
            dma, chunk_sems,
            dma((2,)), dma((2,)),
        ],
        compiler_params=pltpu.CompilerParams(
            collective_id=0, has_side_effects=True, vmem_limit_bytes=int(59.5 * 2**20)
        ),
        name="layer",
    )(
        *small,
        *columns,
        *big,
    )


def solution(mesh):
    finer = Mesh(mesh.devices.reshape(8, 4, 4, mesh.shape["tp"]), ("ep_0", "ep_1", "ep_2", "tp"))
    in_specs = (
        P(EP, None),
        P(EP),
        P(EP, "tp", None, None),
        P(),
        P(),
        P(),
        P(),
        P(EP, "tp"),
        P(EP, "tp"),
        P(EP, "tp"),
        P(EP, "tp"),
        P("tp", EP),
        P(EP, None),
        P(EP, None),
        P(EP, None, "tp"),
        P(EP, None, "tp"),
        P(EP, "tp", None),
        P(None, "tp"),
        P(None, "tp"),
        P("tp", None),
    )
    out_specs = (P(EP, None), P(EP, "tp", None, None))
    return jax.shard_map(
        on_device, mesh=finer, in_specs=in_specs, out_specs=out_specs, check_vma=False
    )
```

```python
import jax
import jax.numpy as jnp
import numpy as np
from jax import lax
from jax.experimental import pallas as pl
from jax.experimental.pallas import tpu as pltpu
from jax.sharding import Mesh
from jax.sharding import PartitionSpec as P

HEAD = 64
HEADS = 16
EP = ("ep_0", "ep_1", "ep_2")
EPS = 1e-06
THETA = 10000.0
MESH = pl.DeviceIdType.MESH
NZ, NY, NX, NG = 8, 4, 4, 16
NCH = 4
PER = 8 // NCH
FAR_FIRST = {
    NZ: sorted(range(NZ), key=lambda step: -min(step, NZ - step)),
    NG: sorted(
        range(NG), key=lambda step: -min(step // 4, 4 - step // 4) - min(step % 4, 4 - step % 4)
    ),
}
BF16 = jnp.bfloat16
F32 = jnp.float32


def place():
    z, y, x, c = (lax.axis_index(name) for name in ("ep_0", "ep_1", "ep_2", "tp"))
    return z, y * NX + x, c


def device(z, g, c):
    return (z, g >> 2, g & 3, c)


def remote(src, dst, send_sem, recv_sem, target):
    return pltpu.make_async_remote_copy(
        src_ref=src,
        dst_ref=dst,
        send_sem=send_sem,
        recv_sem=recv_sem,
        device_id=target,
        device_id_type=MESH,
    )


def each(low, high, body):
    def step(i, carry):
        body(i)
        return carry

    lax.fori_loop(low, high, step, 0)


def dot(a, b, dims=((1,), (0,))):
    return lax.dot_general(a, b, (dims, ((), ())), preferred_element_type=F32)


def wide_rows(blocks):
    rows = blocks.shape[0] * blocks.shape[2]
    return jnp.concatenate(
        [blocks[:, k].reshape(rows, 128) for k in range(blocks.shape[1])], axis=1
    )


def row_scale(blocks):
    count = blocks.shape[0] * blocks.shape[2]
    total = jnp.sum(jnp.sum(blocks * blocks, axis=0), axis=-1, keepdims=True)
    return lax.rsqrt(total / count + EPS)[None]


def arrived(blocks, sem):
    pltpu.make_async_copy(blocks, blocks, sem).wait()


def in_turn(me, size, step):
    if size == NG:
        return ((me + 4 * (step // 4)) & 12) + ((me + step % 4) & 3)
    return (me + step) & (size - 1)


class Exchange:
    def __init__(self, me, size, at, src, dst, send, recv):
        self.me, self.size, self.at, self.src, self.dst = me, size, at, src, dst
        self.send, self.recv = send, recv

    def out(self, step):
        k = in_turn(self.me, self.size, step)
        return remote(self.src(k), self.dst(self.me), self.send, self.recv, self.at(k))

    def start(self, first=1):
        for step in FAR_FIRST[self.size]:
            if step >= first:
                self.out(step).start()


def layer_kernel(
    tokens_hbm, routes_hbm, gates_hbm, lengths_hbm, freq_hbm, mix_hbm, wot_hbm, post_hbm, ffn_hbm, outg_hbm,
    wq_hbm, wk_hbm, wv_hbm, wg_hbm,
    state_hbm, eg_hbm, eu_hbm, ed_hbm, sg_hbm, su_hbm, sd_hbm,
    result_ref, new_hbm,
    state,
    tokens_ref, routes_ref, gates_ref, lengths_ref, freq_ref, mix_ref, wot_ref, post_ref, ffn_ref, outg_ref,
    eg, eu, ed, sg, su, sd,
    wsrc, packed, rt, trig,
    tbuf, abuf, wbuf, zbuf, wo, osend, obuf, qbuf, onehot, comb_hi, comb_lo,
    qt, kt, vsc, fs, decays, rbuf, psend, pbuf, middle, mo, mbuf, shs, shb, ysend, ebuf, ret, back,
    csend, cbuf, mixs, mixb, hid,
    i_s, v_s, w_s, a_s, a_r, t_s, t_r, u_s, u_r, b_s, n_s, b_r, c_s, c_r, d_s, d_r, q_s, q_r,
    o_s, o_r, r_s, r_r, p_s, p_r, m_s, m_r, y_s, y_r, f_s, f_r, g_s, g_r, h_s, h_r, x_s, x_r,
):
    z, g, c = place()
    loads = [
        pltpu.make_async_copy(src, dst, w_s.at[i])
        for i, (src, dst) in enumerate(
            ((state_hbm, state), (sg_hbm, sg), (su_hbm, su), (sd_hbm, sd),
             (eg_hbm, eg), (eu_hbm, eu), (ed_hbm.at[0, :, pl.ds(pl.multiple_of(c * 1024, 128), 1024)], ed.at[c]))
        )
    ]
    barrier = pltpu.get_barrier_semaphore()

    def greet(target):
        pl.semaphore_signal(barrier, inc=1, device_id=target, device_id_type=MESH)

    for step in FAR_FIRST[NZ][:-1]:
        for core in range(2):
            greet(device((z + step) & (NZ - 1), g, core))
    for step in FAR_FIRST[NG]:
        k = in_turn(g, NG, step)
        if step:
            greet(device(z, k, c))
        greet(device(z, k, 1 - c))
    small = [
        pltpu.make_async_copy(src, dst, i_s.at[i])
        for i, (src, dst) in enumerate(
            ((tokens_hbm, tokens_ref), (mix_hbm, mix_ref), (routes_hbm, routes_ref),
             (gates_hbm, gates_ref), (lengths_hbm, lengths_ref), (freq_hbm, freq_ref),
             (wot_hbm, wot_ref), (post_hbm, post_ref), (ffn_hbm, ffn_ref), (outg_hbm, outg_ref))
        )
    ]
    slices = [
        pltpu.make_async_copy(
            w_ref.at[:, pl.ds(k * 128, 128)], wsrc.at[4 * m + k], v_s
        )
        for m, w_ref in enumerate((wq_hbm, wk_hbm, wv_hbm, wg_hbm))
        for k in range(4)
    ]
    for load in slices + small:
        load.start()
    arrived(wsrc, v_s)
    pl.semaphore_wait(barrier, 2 * NG - 1 + 2 * NZ - 2)

    def plane(src, dst, send, recv):
        return Exchange(g, NG, lambda k: device(z, k, c), src, dst, send, recv)

    def column(src, dst, send, recv):
        return Exchange(z, NZ, lambda k: device(k, g, c), src, dst, send, recv)

    others, above = pl.ds(0, NG - 1), pl.ds(0, NZ - 1)

    ga = plane(lambda k: wsrc.at[k], lambda k: abuf.at[k], a_s, a_r)
    gt = plane(lambda k: tbuf.at[c, g], lambda k: tbuf.at[c, k], t_s, t_r.at[g])
    gc = column(lambda k: wot_ref, lambda k: zbuf.at[k], c_s, c_r)
    gq = column(lambda k: rt, lambda k: qbuf.at[k], q_s, q_r)
    ga.start()
    pltpu.make_async_copy(wsrc.at[g], abuf.at[g], a_r).start()
    for load in small[:6]:
        load.wait()
    half = tbuf.shape[-1]
    wide = tokens_ref[...].astype(F32)
    scale = lax.rsqrt(jnp.mean(wide * wide, axis=-1, keepdims=True) + EPS)
    normed = (wide * scale * mix_ref[...]).astype(BF16)
    for k in range(2):
        tbuf[k, pl.ds(g, 1)] = normed[:, k * half : (k + 1) * half][None]
    packed[...] = jnp.zeros_like(packed)
    packed[0:6, 0:16] = routes_ref[...].astype(F32)
    packed[8:14, 0:16] = gates_ref[...]
    packed[14:15, 0:16] = lengths_ref[...].astype(F32)
    turned = packed[...].T[0:16]
    earlier = lax.broadcasted_iota(jnp.int32, (16, 16), 1) < lax.broadcasted_iota(
        jnp.int32, (16, 16), 0
    )
    column_of = lax.broadcasted_iota(jnp.int32, (16, 16), 1)
    table = turned
    for k in range(6):
        same = jnp.zeros((16, 16), F32)
        for other in range(6):
            same = jnp.where(
                turned[:, k : k + 1] == packed[other : other + 1, 0:16], 1.0, same
            )
        rank = jnp.max(jnp.where(earlier, same, 0.0), axis=1, keepdims=True)
        table = jnp.where(column_of == k, turned * 2.0 + rank, table)
    rt[:, 0:16] = table
    gq.start()
    for load in loads:
        load.start()
    swap = remote(
        ed_hbm.at[0, :, pl.ds(pl.multiple_of((1 - c) * 1024, 128), 1024)],
        ed.at[c],
        x_s.at[2],
        x_r.at[2],
        device(z, g, 1 - c),
    )
    swap.start()
    qbuf[pl.ds(z, 1), :, 0:16] = rt[:, 0:16][None]

    arrived(abuf, a_r)

    def b_copy(delta):
        return remote(
            abuf, wbuf.at[z], b_s, b_r.at[z], device((z + delta) & (NZ - 1), g, c)
        )

    for delta in (2, -2, 1, -1):
        b_copy(delta).start()
    pltpu.make_async_copy(abuf, wbuf.at[z], b_r.at[z]).start()
    gt.start()

    def b_wait(delta):
        source = (z + delta) & (NZ - 1)
        pltpu.make_async_copy(abuf, wbuf.at[source], b_r.at[source]).wait()

    def onward(delta, to):
        source = (z + delta) & (NZ - 1)
        return remote(
            wbuf.at[source],
            wbuf.at[source],
            n_s,
            b_r.at[source],
            device((z + to) & (NZ - 1), g, c),
        )

    to_half = g >> 3

    def d_start(k):
        other = 2 * k + to_half

        @pl.when(other == g)
        def _():
            pltpu.make_async_copy(zbuf.at[k], wo.at[g & 7], d_r).start()

        @pl.when(other != g)
        def _():
            remote(zbuf.at[k], wo.at[g & 7], d_s, d_r, device(z, other, c)).start()

    for load in small[6:]:
        load.wait()
    arrived(qbuf.at[above], q_r)
    routing = qbuf[...].reshape(NZ * 16, 128)
    slots = 16 * NG
    row_z = lax.broadcasted_iota(jnp.int32, (NZ * 16, slots), 0) // 16
    lane = lax.broadcasted_iota(jnp.int32, (NZ * 16, slots), 1)
    slot_id = ((z * NG + lane // 16) * 2 + lane % 2).astype(F32)
    same_z = row_z == (lane % 16) // 2
    named = jnp.zeros((NZ * 16, slots), F32)
    weight = jnp.zeros((NZ * 16, slots), F32)
    for k in range(6):
        hit = jnp.logical_and(routing[:, k : k + 1] == slot_id, same_z)
        named = named + jnp.where(hit, 1.0, 0.0)
        weight = weight + jnp.where(hit, routing[:, 8 + k : 9 + k], 0.0)
    onehot[...] = named.T.astype(BF16)
    upper = weight.astype(BF16)
    comb_hi[...] = upper
    comb_lo[...] = (weight - upper.astype(F32)).astype(BF16)

    angles = rt[:, 14:15] * freq_ref[...]
    first = lax.broadcasted_iota(jnp.int32, (16, 128), 1) % 64 < 32
    trig[0] = jnp.cos(angles)
    sines = jnp.sin(angles)
    trig[1] = jnp.where(first, -sines, sines)
    heads = lax.broadcasted_iota(jnp.int32, (8, 128), 0) + c * 8
    decays[...] = 1.0 - jnp.exp2(-5.0 - 7.0 * heads.astype(F32) / (HEADS - 1))
    b_wait(-2)
    onward(-2, 2).start()
    onward(-2, 1).start()
    b_wait(2)
    onward(2, -1).start()

    def t_forward(half_of, k):
        block = tbuf.at[half_of, k]
        return remote(block, block, u_s, u_r, device(z, g, 1 - c))

    for step in FAR_FIRST[NG][:-1]:
        k = in_turn(g, NG, step)
        arrived(tbuf.at[c, k], t_r.at[k])
        t_forward(c, k).start()
    arrived(tbuf.at[1 - c, others], u_r)

    for delta in (0, 1, -1, 3, -3, 4):
        b_wait(delta)
    rows = NG * tbuf.shape[2]
    mine = dot(tbuf[0].reshape(rows, half), wbuf[0:4].reshape(half, 128)) + dot(
        tbuf[1].reshape(rows, half), wbuf[4:8].reshape(half, 128)
    )
    osend[...] = mine.astype(BF16).reshape(osend.shape)
    go = plane(lambda k: osend.at[k], lambda k: obuf.at[k], o_s, o_r)
    go.start()
    gc = column(lambda k: wot_ref, lambda k: zbuf.at[z], c_s, c_r)
    gc.start()
    pltpu.make_async_copy(wot_ref, zbuf.at[z], c_r).start()
    obuf[pl.ds(g, 1)] = osend[pl.ds(g, 1)]
    arrived(abuf.at[others], a_s)
    arrived(tbuf.at[c, others], t_s)
    arrived(tbuf.at[c, others], u_s)
    arrived(qbuf.at[above], q_s)
    arrived(wbuf.at[pl.ds(0, 4)], b_s)
    arrived(wbuf.at[pl.ds(0, 3)], n_s)
    loads[0].wait()
    arrived(obuf.at[others], o_r)
    arrived(zbuf, c_r)
    each(0, NZ, d_start)
    low_half = lax.broadcasted_iota(jnp.int32, (16, 128), 1) < 64
    def rotate(v):
        other = jnp.where(first, pltpu.roll(v, 96, 1), pltpu.roll(v, 32, 1))
        return v * trig[0] + other * trig[1]

    def by_head(v):
        low = jnp.sum(jnp.where(low_half, v, 0.0), axis=-1, keepdims=True)
        high = jnp.sum(jnp.where(low_half, 0.0, v), axis=-1, keepdims=True)
        return jnp.where(low_half, low, high)

    def block(k, hp):
        return obuf[4 * k + hp].astype(F32)

    self_terms = []
    for hp in range(4):
        query = rotate(block(0, hp))
        key = rotate(block(1, hp)) * HEAD ** (-0.5)
        value = block(2, hp)
        qt[hp] = query.T
        kt[hp] = key.T
        vsc[2 * hp] = value
        vsc[2 * hp + 1] = pltpu.roll(value, 64, 1)
        self_terms.append(by_head(query * key) * value)

    def read_pair(hp):
        queries = qt[pl.ds(hp, 1)][0]
        for h in range(2):
            for s in range(16):
                held = state[s, pl.ds(2 * hp + h, 1)][0]
                column_q = queries[h * 64 : (h + 1) * 64, s : s + 1]
                fs[pl.ds(2 * hp + h, 1), s : s + 1, 0:64] = jnp.sum(
                    column_q * held, axis=0, keepdims=True
                )[None]

    for part in range(2):
        each(2 * part, 2 * part + 2, read_pair)
        for hp in (2 * part, 2 * part + 1):
            from_state = jnp.where(low_half, fs[2 * hp], pltpu.roll(fs[2 * hp + 1], 64, 1))
            decay = jnp.where(
                low_half[0:1], decays[2 * hp : 2 * hp + 1], decays[2 * hp + 1 : 2 * hp + 2]
            )
            read = decay * from_state + self_terms[hp]
            read = read * lax.rsqrt(by_head(read * read) / HEAD + EPS)
            rbuf[part, pl.ds(g, 1), hp & 1] = (read * jax.nn.silu(block(3, hp))).astype(BF16)[None]
        plane(
            lambda k, part=part: rbuf.at[part, g], lambda k, part=part: rbuf.at[part, g], r_s, r_r
        ).start()

    def update_pair(hp):
        keys = kt[pl.ds(hp, 1)][0]
        for h in range(2):
            decay = decays[pl.ds(2 * hp + h, 1), 0:64]
            value = vsc[pl.ds(2 * hp + h, 1)][0]
            for s in range(16):
                held = state[s, pl.ds(2 * hp + h, 1)][0]
                column_k = keys[h * 64 : (h + 1) * 64, s : s + 1]
                state[s, pl.ds(2 * hp + h, 1)] = (
                    decay * held + column_k * value[s : s + 1, 0:64]
                )[None]

    each(0, 4, update_pair)
    def d_wait(k):
        pltpu.make_async_copy(zbuf.at[k], wo.at[k], d_r.at[k]).wait()

    store = pltpu.make_async_copy(state, new_hbm, w_s.at[7])
    store.start()
    arrived(obuf.at[others], o_s)
    arrived(zbuf.at[above], c_s)

    @pl.when((g & 1) == to_half)
    def _():
        arrived(zbuf.at[above], d_s)

    @pl.when((g & 1) != to_half)
    def _():
        arrived(zbuf, d_s)

    arrived(wo, d_r)
    arrived(rbuf.at[:, others], r_r)
    partial = dot(
        jnp.concatenate([wide_rows(rbuf[0]), wide_rows(rbuf[1])], axis=1),
        wo[...].reshape(128, 512),
        ((1,), (1,)),
    )
    psend[...] = partial.astype(BF16).reshape(psend.shape)
    gp = plane(lambda k: psend.at[k], lambda k: pbuf.at[c, k], p_s.at[0], p_r.at[0])
    gp_other = Exchange(
        g, NG, lambda k: device(z, k, 1 - c), lambda k: psend.at[k], lambda k: pbuf.at[c, k],
        p_s.at[1], p_r.at[1],
    )
    for step in FAR_FIRST[NG]:
        if step:
            gp.out(step).start()
        gp_other.out(step).start()
    pbuf[pl.ds(c, 1), pl.ds(g, 1)] = psend[pl.ds(g, 1)][None]
    arrived(rbuf.at[:, others], r_s)
    arrived(psend.at[others], p_r.at[0])
    arrived(psend, p_r.at[1])
    mixed = (pbuf[0].astype(F32) + pbuf[1].astype(F32)).astype(BF16).astype(F32)
    tok = jnp.stack([tokens_ref[:, k * 128 : (k + 1) * 128] for k in range(NG)]).astype(F32)
    mid = (tok + mixed * row_scale(mixed) * post_ref[...]).astype(BF16)
    middle[...] = mid
    mid = mid.astype(F32)
    mo[...] = (mid * row_scale(mid) * ffn_ref[...]).astype(BF16)

    for n in range(NCH):
        blocks = pl.ds(c * 8 + n * PER, PER)
        mbuf[n, pl.ds(z, 1)] = mo[blocks][None]
        gm = column(lambda k, n=n: mbuf.at[n, z], lambda k, n=n: mbuf.at[n, k], m_s, m_r.at[n])
        gm.start()
    for load in loads[1:4]:
        load.wait()
    rows_in = wide_rows(mo[...][None])
    shared_hidden = (jax.nn.silu(dot(rows_in, sg[...])) * dot(rows_in, su[...])).astype(BF16)
    shared_part = dot(shared_hidden, sd[...]).astype(BF16)
    parts = jnp.stack([shared_part[:, k * 128 : (k + 1) * 128] for k in range(NG)])
    shs[...] = parts.reshape(shs.shape)
    share = remote(shs.at[1 - c], shb, x_s.at[0], x_r.at[0], device(z, g, 1 - c))
    share.start()
    for load in loads[4:]:
        load.wait()
    swap.wait_send()
    arrived(ed.at[1 - c], x_r.at[2])
    arrived(psend.at[others], p_s.at[0])
    arrived(psend, p_s.at[1])
    for n in range(NCH):
        arrived(mbuf.at[n, above], m_r.at[n])
        sorted_rows = dot(onehot[...], wide_rows(mbuf[n])).astype(BF16)
        for k in range(PER):
            ysend[n, :, k] = sorted_rows[:, k * 128 : (k + 1) * 128].reshape(NG, 16, 128)
        gy = plane(lambda k, n=n: ysend.at[n, k], lambda k, n=n: ebuf.at[n, c, k], y_s, y_r.at[n])
        gy.start()
        ebuf[n, pl.ds(c, 1), pl.ds(g, 1)] = ysend[n, pl.ds(g, 1)][None]
    arrived(mbuf.at[:, above], m_s)

    def forward(n):
        rows = ebuf.at[n, c]
        return remote(rows, rows, f_s.at[n], f_r.at[n], device(z, g, 1 - c))

    def expert_in(n, k):
        blocks = wide_rows(ebuf[n, pl.ds(k, 1)][0])
        rows_of = pl.ds(pl.multiple_of(k * half + n * PER * 128, 128), PER * 128)
        return dot(blocks, eg[0, rows_of]), dot(blocks, eu[0, rows_of])

    gates, ups = [], []
    for n in range(NCH):
        arrived(ebuf.at[n, c, others], y_r.at[n])
        forward(n).start()
        gate, up = expert_in(n, c)
        gates.append(gate)
        ups.append(up)
    for n in range(NCH):
        arrived(ebuf.at[n, 1 - c], f_r.at[n])
        gate, up = expert_in(n, 1 - c)
        gates.append(gate)
        ups.append(up)
    hid[pl.ds(c, 1)] = (jax.nn.silu(sum(gates)) * sum(ups)).astype(BF16)[None]
    give = remote(hid.at[c], hid.at[c], x_s.at[3], x_r.at[3], device(z, g, 1 - c))
    give.start()
    arrived(hid.at[1 - c], x_r.at[3])
    hidden = jnp.concatenate([hid[0], hid[1]], axis=1)
    for n in range(NCH):
        cols_of = slice(n * PER * 128, (n + 1) * PER * 128)
        rows_out = dot(hidden, ed[:, :, cols_of].reshape(512, PER * 128)).astype(BF16)
        for j in range(PER):
            ret[n, :, j] = rows_out[:, j * 128 : (j + 1) * 128].reshape(NG, 16, 128)
        gg = plane(lambda k, n=n: ret.at[n, k], lambda k, n=n: back.at[n, k], g_s, g_r.at[n])
        gg.start()
        back[n, pl.ds(g, 1)] = ret[n, pl.ds(g, 1)]
    share.wait_recv()
    shared_out = (shs[pl.ds(c, 1)][0].astype(F32) + shb[...].astype(F32)).astype(BF16).astype(F32)
    arrived(ysend.at[:, others], y_s)
    for n in range(NCH):
        forward(n).wait_send()
    give.wait_send()
    share.wait_send()

    for n in range(NCH):
        arrived(back.at[n, others], g_r.at[n])
        answers = wide_rows(back[n])
        sums = (dot(comb_hi[...], answers) + dot(comb_lo[...], answers)).astype(BF16)
        for k in range(PER):
            csend[n, :, k] = sums[:, k * 128 : (k + 1) * 128].reshape(NZ, 16, 128)
        gh = column(lambda k, n=n: csend.at[n, k], lambda k, n=n: cbuf.at[n, k], h_s, h_r.at[n])
        gh.start()
        cbuf[n, pl.ds(z, 1)] = csend[n, pl.ds(z, 1)]
    arrived(ret.at[:, others], g_s)
    for n in range(NCH):
        arrived(cbuf.at[n, above], h_r.at[n])
        part = slice(n * PER, (n + 1) * PER)
        mixs[part] = shared_out[part] + jnp.sum(cbuf[n].astype(F32), axis=0)
    last = remote(mixs, mixb, x_s.at[1], x_r.at[1], device(z, g, 1 - c))
    last.start()
    last.wait_recv()
    first_half = jnp.where(c == 0, mixs[...], mixb[...])
    second_half = jnp.where(c == 0, mixb[...], mixs[...])
    mixture = jnp.concatenate([first_half, second_half], axis=0)
    final = (middle[...].astype(F32) + mixture * row_scale(mixture) * outg_ref[...]).astype(BF16)
    for k in range(NG):
        result_ref[:, k * 128 : (k + 1) * 128] = final[k]
    arrived(csend.at[:, above], h_s)
    last.wait_send()
    store.wait()


def on_device(
    tokens, lengths, prior_state, mix_gain, post_gain, ffn_gain, out_gain,
    query_weight, key_weight, value_weight, gate_weight, out_weight, routes, route_gates,
    expert_gate, expert_up, expert_down, shared_gate, shared_up, shared_down,
):
    seq, width = tokens.shape
    frequency = THETA ** (-(np.arange(128) % 32).astype(np.float64) / 32)
    dma = pltpu.SemaphoreType.DMA
    blocks = pltpu.VMEM((NG, 16, 128), BF16)
    halves = pltpu.VMEM((NCH, NG, PER, 16, 128), BF16)
    columns_of = pltpu.VMEM((NCH, NZ, PER, 16, 128), BF16)
    vmem = pl.BlockSpec(memory_space=pltpu.VMEM)
    anywhere = pl.BlockSpec(memory_space=pl.ANY)
    big = (prior_state, expert_gate, expert_up, expert_down, shared_gate, shared_up, shared_down)
    chunk_sems = dma((NCH,))
    post, ffn, outer = (gain.reshape(NG, 1, 128) for gain in (post_gain, ffn_gain, out_gain))
    small = (
        tokens, routes.T, route_gates.T, lengths[None], jnp.asarray(frequency[None], F32),
        mix_gain[None], out_weight.T, post, ffn, outer,
    )
    columns = (query_weight, key_weight, value_weight, gate_weight)
    return pl.pallas_call(
        layer_kernel,
        out_shape=(
            pltpu.VMEM((seq, width), BF16),
            pltpu.VMEM(prior_state.shape, F32),
        ),
        in_specs=[anywhere] * (len(small) + len(columns) + len(big)),
        out_specs=(vmem, anywhere),
        scratch_shapes=[
            pltpu.VMEM(prior_state.shape, F32),
            *(pltpu.VMEM(array.shape, array.dtype) for array in small + big[1:3]),
            pltpu.VMEM((2, 256, 1024), BF16),
            *(pltpu.VMEM(array.shape, array.dtype) for array in big[4:]),
            blocks,
            pltpu.VMEM((16, 128), F32),
            pltpu.VMEM((16, 128), F32),
            pltpu.VMEM((2, 16, 128), F32),
            pltpu.VMEM((2, NG, seq, width // 2), BF16),
            blocks,
            pltpu.VMEM((NZ, NG, 16, 128), BF16),
            pltpu.VMEM((8, 16, 512), BF16),
            pltpu.VMEM((8, 16, 512), BF16),
            blocks,
            blocks,
            pltpu.VMEM((NZ, 16, 128), F32),
            pltpu.VMEM((16 * NG, 16 * NZ), BF16),
            pltpu.VMEM((16 * NZ, 16 * NG), BF16),
            pltpu.VMEM((16 * NZ, 16 * NG), BF16),
            pltpu.VMEM((4, 128, 16), F32),
            pltpu.VMEM((4, 128, 16), F32),
            pltpu.VMEM((8, 16, 128), F32),
            pltpu.VMEM((8, 16, 128), F32),
            pltpu.VMEM((8, 128), F32),
            pltpu.VMEM((2, NG, 2, 16, 128), BF16),
            blocks,
            pltpu.VMEM((2, NG, 16, 128), BF16),
            blocks,
            blocks,
            columns_of,
            pltpu.VMEM((2, 8, 16, 128), BF16),
            pltpu.VMEM((8, 16, 128), BF16),
            halves,
            pltpu.VMEM((NCH, 2, NG, PER, 16, 128), BF16),
            halves,
            halves,
            columns_of,
            columns_of,
            pltpu.VMEM((8, 16, 128), F32),
            pltpu.VMEM((8, 16, 128), F32),
            pltpu.VMEM((2, 256, 256), BF16),
            dma((len(small),)),
            dma,
            dma((8,)),
            dma, dma,
            dma, dma((NG,)),
            dma, dma,
            dma, dma, dma((NZ,)),
            dma, dma, dma, dma, dma, dma,
            dma, dma, dma, dma,
            dma((2,)), dma((2,)),
            dma, chunk_sems,
            dma, chunk_sems,
            chunk_sems, chunk_sems,
            dma, chunk_sems,
            dma, chunk_sems,
            dma((4,)), dma((4,)),
        ],
        compiler_params=pltpu.CompilerParams(
            collective_id=0, has_side_effects=True, vmem_limit_bytes=int(59.5 * 2**20)
        ),
        name="layer",
    )(
        *small,
        *columns,
        *big,
    )


def solution(mesh):
    finer = Mesh(mesh.devices.reshape(8, 4, 4, mesh.shape["tp"]), ("ep_0", "ep_1", "ep_2", "tp"))
    in_specs = (
        P(EP, None),
        P(EP),
        P(EP, "tp", None, None),
        P(),
        P(),
        P(),
        P(),
        P(EP, "tp"),
        P(EP, "tp"),
        P(EP, "tp"),
        P(EP, "tp"),
        P("tp", EP),
        P(EP, None),
        P(EP, None),
        P(EP, None, "tp"),
        P(EP, None, "tp"),
        P(EP, "tp", None),
        P(None, "tp"),
        P(None, "tp"),
        P("tp", None),
    )
    out_specs = (P(EP, None), P(EP, "tp", None, None))
    return jax.shard_map(
        on_device, mesh=finer, in_specs=in_specs, out_specs=out_specs, check_vma=False
    )
```

```python
import jax
import jax.numpy as jnp
import numpy as np
from jax import lax
from jax.experimental import pallas as pl
from jax.experimental.pallas import tpu as pltpu
from jax.sharding import Mesh
from jax.sharding import PartitionSpec as P

HEAD = 64
HEADS = 16
EP = ("ep_0", "ep_1", "ep_2")
EPS = 1e-06
THETA = 10000.0
MESH = pl.DeviceIdType.MESH
NZ, NY, NX, NG = 8, 4, 4, 16
NCH = 4
PER = 8 // NCH
FAR_FIRST = {
    NZ: sorted(range(NZ), key=lambda step: -min(step, NZ - step)),
    NG: sorted(
        range(NG), key=lambda step: -min(step // 4, 4 - step // 4) - min(step % 4, 4 - step % 4)
    ),
}
BF16 = jnp.bfloat16
F32 = jnp.float32


def place():
    z, y, x, c = (lax.axis_index(name) for name in ("ep_0", "ep_1", "ep_2", "tp"))
    return z, y * NX + x, c


def device(z, g, c):
    return (z, g >> 2, g & 3, c)


def remote(src, dst, send_sem, recv_sem, target):
    return pltpu.make_async_remote_copy(
        src_ref=src,
        dst_ref=dst,
        send_sem=send_sem,
        recv_sem=recv_sem,
        device_id=target,
        device_id_type=MESH,
    )


def each(low, high, body):
    def step(i, carry):
        body(i)
        return carry

    lax.fori_loop(low, high, step, 0)


def dot(a, b, dims=((1,), (0,))):
    return lax.dot_general(a, b, (dims, ((), ())), preferred_element_type=F32)


def wide_rows(blocks):
    rows = blocks.shape[0] * blocks.shape[2]
    return jnp.concatenate(
        [blocks[:, k].reshape(rows, 128) for k in range(blocks.shape[1])], axis=1
    )


def row_scale(blocks):
    count = blocks.shape[0] * blocks.shape[2]
    total = jnp.sum(jnp.sum(blocks * blocks, axis=0), axis=-1, keepdims=True)
    return lax.rsqrt(total / count + EPS)[None]


def arrived(blocks, sem):
    pltpu.make_async_copy(blocks, blocks, sem).wait()


def in_turn(me, size, step):
    if size == NG:
        return ((me + 4 * (step // 4)) & 12) + ((me + step % 4) & 3)
    return (me + step) & (size - 1)


class Exchange:
    def __init__(self, me, size, at, src, dst, send, recv):
        self.me, self.size, self.at, self.src, self.dst = me, size, at, src, dst
        self.send, self.recv = send, recv

    def out(self, step):
        k = in_turn(self.me, self.size, step)
        return remote(self.src(k), self.dst(self.me), self.send, self.recv, self.at(k))

    def start(self, first=1):
        for step in FAR_FIRST[self.size]:
            if step >= first:
                self.out(step).start()


def layer_kernel(
    tokens_hbm, routes_hbm, gates_hbm, lengths_hbm, freq_hbm, mix_hbm, wot_hbm, post_hbm, ffn_hbm, outg_hbm,
    wq_hbm, wk_hbm, wv_hbm, wg_hbm,
    state_hbm, eg_hbm, eu_hbm, ed_hbm, sg_hbm, su_hbm, sd_hbm,
    result_ref, new_hbm,
    state,
    tokens_ref, routes_ref, gates_ref, lengths_ref, freq_ref, mix_ref, wot_ref, post_ref, ffn_ref, outg_ref,
    eg, eu, ed, sg, su, sd,
    wsrc, packed, rt, trig,
    tbuf, abuf, wbuf, zbuf, wo, osend, obuf, qbuf, onehot, comb_hi, comb_lo,
    qt, kt, vsc, fs, decays, rbuf, psend, pbuf, middle, mo, mbuf, shs, shb, ysend, ebuf, ret, back,
    csend, cbuf, mixs, mixb,
    i_s, v_s, w_s, a_s, a_r, t_s, t_r, u_s, u_r, b_s, n_s, b_r, c_s, c_r, d_s, d_r, q_s, q_r,
    o_s, o_r, r_s, r_r, p_s, p_r, m_s, m_r, y_s, y_r, g_s, g_r, h_s, h_r, x_s, x_r,
):
    z, g, c = place()
    loads = [
        pltpu.make_async_copy(src, dst, w_s.at[i])
        for i, (src, dst) in enumerate(
            ((state_hbm, state), (sg_hbm, sg), (su_hbm, su), (sd_hbm, sd),
             (eg_hbm.at[0], eg.at[c]), (eu_hbm.at[0], eu.at[c]), (ed_hbm.at[0], ed.at[c]))
        )
    ]
    barrier = pltpu.get_barrier_semaphore()

    def greet(target):
        pl.semaphore_signal(barrier, inc=1, device_id=target, device_id_type=MESH)

    for step in FAR_FIRST[NZ][:-1]:
        for core in range(2):
            greet(device((z + step) & (NZ - 1), g, core))
    for step in FAR_FIRST[NG]:
        k = in_turn(g, NG, step)
        if step:
            greet(device(z, k, c))
        greet(device(z, k, 1 - c))
    small = [
        pltpu.make_async_copy(src, dst, i_s.at[i])
        for i, (src, dst) in enumerate(
            ((tokens_hbm, tokens_ref), (mix_hbm, mix_ref), (routes_hbm, routes_ref),
             (gates_hbm, gates_ref), (lengths_hbm, lengths_ref), (freq_hbm, freq_ref),
             (wot_hbm, wot_ref), (post_hbm, post_ref), (ffn_hbm, ffn_ref), (outg_hbm, outg_ref))
        )
    ]
    slices = [
        pltpu.make_async_copy(
            w_ref.at[:, pl.ds(k * 128, 128)], wsrc.at[4 * m + k], v_s
        )
        for m, w_ref in enumerate((wq_hbm, wk_hbm, wv_hbm, wg_hbm))
        for k in range(4)
    ]
    for load in slices + small:
        load.start()
    arrived(wsrc, v_s)
    pl.semaphore_wait(barrier, 2 * NG - 1 + 2 * NZ - 2)

    def plane(src, dst, send, recv):
        return Exchange(g, NG, lambda k: device(z, k, c), src, dst, send, recv)

    def column(src, dst, send, recv):
        return Exchange(z, NZ, lambda k: device(k, g, c), src, dst, send, recv)

    others, above = pl.ds(0, NG - 1), pl.ds(0, NZ - 1)

    ga = plane(lambda k: wsrc.at[k], lambda k: abuf.at[k], a_s, a_r)
    gt = plane(lambda k: tbuf.at[c, g], lambda k: tbuf.at[c, k], t_s, t_r.at[g])
    gc = column(lambda k: wot_ref, lambda k: zbuf.at[k], c_s, c_r)
    gq = column(lambda k: rt, lambda k: qbuf.at[k], q_s, q_r)
    ga.start()
    pltpu.make_async_copy(wsrc.at[g], abuf.at[g], a_r).start()
    for load in small[:6]:
        load.wait()
    half = tbuf.shape[-1]
    wide = tokens_ref[...].astype(F32)
    scale = lax.rsqrt(jnp.mean(wide * wide, axis=-1, keepdims=True) + EPS)
    normed = (wide * scale * mix_ref[...]).astype(BF16)
    for k in range(2):
        tbuf[k, pl.ds(g, 1)] = normed[:, k * half : (k + 1) * half][None]
    packed[...] = jnp.zeros_like(packed)
    packed[0:6, 0:16] = routes_ref[...].astype(F32)
    packed[8:14, 0:16] = gates_ref[...]
    packed[14:15, 0:16] = lengths_ref[...].astype(F32)
    turned = packed[...].T[0:16]
    earlier = lax.broadcasted_iota(jnp.int32, (16, 16), 1) < lax.broadcasted_iota(
        jnp.int32, (16, 16), 0
    )
    column_of = lax.broadcasted_iota(jnp.int32, (16, 16), 1)
    table = turned
    for k in range(6):
        same = jnp.zeros((16, 16), F32)
        for other in range(6):
            same = jnp.where(
                turned[:, k : k + 1] == packed[other : other + 1, 0:16], 1.0, same
            )
        rank = jnp.max(jnp.where(earlier, same, 0.0), axis=1, keepdims=True)
        table = jnp.where(column_of == k, turned * 2.0 + rank, table)
    rt[:, 0:16] = table
    gq.start()
    for load in loads:
        load.start()
    qbuf[pl.ds(z, 1), :, 0:16] = rt[:, 0:16][None]

    arrived(abuf, a_r)

    def part_of(array, half_of):
        return array.at[pl.ds(half_of * 8, 8)]

    def b_copy(delta, half_of):
        return remote(
            part_of(abuf, half_of),
            part_of(wbuf.at[z], half_of),
            b_s,
            b_r.at[z, half_of],
            device((z + delta) & (NZ - 1), g, c),
        )

    for delta, half_of in ((2, 0), (-2, 0), (2, 1), (-2, 1), (1, 0), (-1, 0), (1, 1), (-1, 1)):
        b_copy(delta, half_of).start()
    for half_of in range(2):
        pltpu.make_async_copy(
            part_of(abuf, half_of), part_of(wbuf.at[z], half_of), b_r.at[z, half_of]
        ).start()
    gt.start()

    def b_wait(delta, half_of):
        source = (z + delta) & (NZ - 1)
        arrived(part_of(wbuf.at[source], half_of), b_r.at[source, half_of])

    def onward(delta, to, half_of):
        source = (z + delta) & (NZ - 1)
        block = part_of(wbuf.at[source], half_of)
        return remote(
            block, block, n_s, b_r.at[source, half_of], device((z + to) & (NZ - 1), g, c)
        )

    to_half = g >> 3

    def d_start(k):
        other = 2 * k + to_half

        @pl.when(other == g)
        def _():
            pltpu.make_async_copy(zbuf.at[k], wo.at[g & 7], d_r).start()

        @pl.when(other != g)
        def _():
            remote(zbuf.at[k], wo.at[g & 7], d_s, d_r, device(z, other, c)).start()

    for load in small[6:]:
        load.wait()
    arrived(qbuf.at[above], q_r)
    routing = qbuf[...].reshape(NZ * 16, 128)
    slots = 16 * NG
    row_z = lax.broadcasted_iota(jnp.int32, (NZ * 16, slots), 0) // 16
    lane = lax.broadcasted_iota(jnp.int32, (NZ * 16, slots), 1)
    slot_id = ((z * NG + lane // 16) * 2 + lane % 2).astype(F32)
    same_z = row_z == (lane % 16) // 2
    named = jnp.zeros((NZ * 16, slots), F32)
    weight = jnp.zeros((NZ * 16, slots), F32)
    for k in range(6):
        hit = jnp.logical_and(routing[:, k : k + 1] == slot_id, same_z)
        named = named + jnp.where(hit, 1.0, 0.0)
        weight = weight + jnp.where(hit, routing[:, 8 + k : 9 + k], 0.0)
    onehot[...] = named.T.astype(BF16)
    upper = weight.astype(BF16)
    comb_hi[...] = upper
    comb_lo[...] = (weight - upper.astype(F32)).astype(BF16)

    angles = rt[:, 14:15] * freq_ref[...]
    first = lax.broadcasted_iota(jnp.int32, (16, 128), 1) % 64 < 32
    trig[0] = jnp.cos(angles)
    sines = jnp.sin(angles)
    trig[1] = jnp.where(first, -sines, sines)
    heads = lax.broadcasted_iota(jnp.int32, (8, 128), 0) + c * 8
    decays[...] = 1.0 - jnp.exp2(-5.0 - 7.0 * heads.astype(F32) / (HEADS - 1))
    for half_of in range(2):
        b_wait(-2, half_of)
        onward(-2, 2, half_of).start()
        onward(-2, 1, half_of).start()
        b_wait(2, half_of)
        onward(2, -1, half_of).start()

    def t_forward(half_of, k):
        block = tbuf.at[half_of, k]
        return remote(block, block, u_s, u_r, device(z, g, 1 - c))

    for step in FAR_FIRST[NG][:-1]:
        k = in_turn(g, NG, step)
        arrived(tbuf.at[c, k], t_r.at[k])
        t_forward(c, k).start()
    arrived(tbuf.at[1 - c, others], u_r)

    for delta in (0, 1, -1, 3, -3, 4):
        b_wait(delta, 0)
        b_wait(delta, 1)
    rows = NG * tbuf.shape[2]
    mine = dot(tbuf[0].reshape(rows, half), wbuf[0:4].reshape(half, 128)) + dot(
        tbuf[1].reshape(rows, half), wbuf[4:8].reshape(half, 128)
    )
    osend[...] = mine.astype(BF16).reshape(osend.shape)
    go = plane(lambda k: osend.at[k], lambda k: obuf.at[k], o_s, o_r)
    go.start()
    swaps = [
        remote(src.at[0], dst.at[c], x_s.at[2 + i], x_r.at[2 + i], device(z, g, 1 - c))
        for i, (src, dst) in enumerate(((eg_hbm, eg), (eu_hbm, eu), (ed_hbm, ed)))
    ]
    for swap in swaps:
        swap.start()
    gc = column(lambda k: wot_ref, lambda k: zbuf.at[z], c_s, c_r)
    gc.start()
    pltpu.make_async_copy(wot_ref, zbuf.at[z], c_r).start()
    obuf[pl.ds(g, 1)] = osend[pl.ds(g, 1)]
    arrived(abuf.at[others], a_s)
    arrived(tbuf.at[c, others], t_s)
    arrived(tbuf.at[c, others], u_s)
    arrived(qbuf.at[above], q_s)
    arrived(wbuf.at[pl.ds(0, 4)], b_s)
    arrived(wbuf.at[pl.ds(0, 3)], n_s)
    loads[0].wait()
    arrived(obuf.at[others], o_r)
    arrived(zbuf, c_r)
    each(0, NZ, d_start)
    low_half = lax.broadcasted_iota(jnp.int32, (16, 128), 1) < 64
    def rotate(v):
        other = jnp.where(first, pltpu.roll(v, 96, 1), pltpu.roll(v, 32, 1))
        return v * trig[0] + other * trig[1]

    def by_head(v):
        low = jnp.sum(jnp.where(low_half, v, 0.0), axis=-1, keepdims=True)
        high = jnp.sum(jnp.where(low_half, 0.0, v), axis=-1, keepdims=True)
        return jnp.where(low_half, low, high)

    def block(k, hp):
        return obuf[4 * k + hp].astype(F32)

    self_terms = []
    for hp in range(4):
        query = rotate(block(0, hp))
        key = rotate(block(1, hp)) * HEAD ** (-0.5)
        value = block(2, hp)
        qt[hp] = query.T
        kt[hp] = key.T
        vsc[2 * hp] = value
        vsc[2 * hp + 1] = pltpu.roll(value, 64, 1)
        self_terms.append(by_head(query * key) * value)

    def read_pair(hp):
        queries = qt[pl.ds(hp, 1)][0]
        for h in range(2):
            for s in range(16):
                held = state[s, pl.ds(2 * hp + h, 1)][0]
                column_q = queries[h * 64 : (h + 1) * 64, s : s + 1]
                fs[pl.ds(2 * hp + h, 1), s : s + 1, 0:64] = jnp.sum(
                    column_q * held, axis=0, keepdims=True
                )[None]

    for part in range(2):
        each(2 * part, 2 * part + 2, read_pair)
        for hp in (2 * part, 2 * part + 1):
            from_state = jnp.where(low_half, fs[2 * hp], pltpu.roll(fs[2 * hp + 1], 64, 1))
            decay = jnp.where(
                low_half[0:1], decays[2 * hp : 2 * hp + 1], decays[2 * hp + 1 : 2 * hp + 2]
            )
            read = decay * from_state + self_terms[hp]
            read = read * lax.rsqrt(by_head(read * read) / HEAD + EPS)
            rbuf[part, pl.ds(g, 1), hp & 1] = (read * jax.nn.silu(block(3, hp))).astype(BF16)[None]
        plane(
            lambda k, part=part: rbuf.at[part, g], lambda k, part=part: rbuf.at[part, g], r_s, r_r
        ).start()

    def update_pair(hp):
        keys = kt[pl.ds(hp, 1)][0]
        for h in range(2):
            decay = decays[pl.ds(2 * hp + h, 1), 0:64]
            value = vsc[pl.ds(2 * hp + h, 1)][0]
            for s in range(16):
                held = state[s, pl.ds(2 * hp + h, 1)][0]
                column_k = keys[h * 64 : (h + 1) * 64, s : s + 1]
                state[s, pl.ds(2 * hp + h, 1)] = (
                    decay * held + column_k * value[s : s + 1, 0:64]
                )[None]

    each(0, 4, update_pair)
    def d_wait(k):
        pltpu.make_async_copy(zbuf.at[k], wo.at[k], d_r.at[k]).wait()

    store = pltpu.make_async_copy(state, new_hbm, w_s.at[7])
    store.start()
    arrived(obuf.at[others], o_s)
    arrived(zbuf.at[above], c_s)

    @pl.when((g & 1) == to_half)
    def _():
        arrived(zbuf.at[above], d_s)

    @pl.when((g & 1) != to_half)
    def _():
        arrived(zbuf, d_s)

    arrived(wo, d_r)
    arrived(rbuf.at[:, others], r_r)
    partial = dot(
        jnp.concatenate([wide_rows(rbuf[0]), wide_rows(rbuf[1])], axis=1),
        wo[...].reshape(128, 512),
        ((1,), (1,)),
    )
    psend[...] = partial.astype(BF16).reshape(psend.shape)
    gp = plane(lambda k: psend.at[k], lambda k: pbuf.at[c, k], p_s.at[0], p_r.at[0])
    gp_other = Exchange(
        g, NG, lambda k: device(z, k, 1 - c), lambda k: psend.at[k], lambda k: pbuf.at[c, k],
        p_s.at[1], p_r.at[1],
    )
    for step in FAR_FIRST[NG]:
        if step:
            gp.out(step).start()
        gp_other.out(step).start()
    pbuf[pl.ds(c, 1), pl.ds(g, 1)] = psend[pl.ds(g, 1)][None]
    arrived(rbuf.at[:, others], r_s)
    arrived(psend.at[others], p_r.at[0])
    arrived(psend, p_r.at[1])
    mixed = (pbuf[0].astype(F32) + pbuf[1].astype(F32)).astype(BF16).astype(F32)
    tok = jnp.stack([tokens_ref[:, k * 128 : (k + 1) * 128] for k in range(NG)]).astype(F32)
    mid = (tok + mixed * row_scale(mixed) * post_ref[...]).astype(BF16)
    middle[...] = mid
    mid = mid.astype(F32)
    mo[...] = (mid * row_scale(mid) * ffn_ref[...]).astype(BF16)

    for n in range(NCH):
        blocks = pl.ds(c * 8 + n * PER, PER)
        mbuf[n, pl.ds(z, 1)] = mo[blocks][None]
        gm = column(lambda k, n=n: mbuf.at[n, z], lambda k, n=n: mbuf.at[n, k], m_s, m_r.at[n])
        gm.start()
    for load in loads[1:4]:
        load.wait()
    rows_in = wide_rows(mo[...][None])
    shared_hidden = (jax.nn.silu(dot(rows_in, sg[...])) * dot(rows_in, su[...])).astype(BF16)
    shared_part = dot(shared_hidden, sd[...]).astype(BF16)
    parts = jnp.stack([shared_part[:, k * 128 : (k + 1) * 128] for k in range(NG)])
    shs[...] = parts.reshape(shs.shape)
    share = remote(shs.at[1 - c], shb, x_s.at[0], x_r.at[0], device(z, g, 1 - c))
    share.start()
    for load in loads[4:]:
        load.wait()
    for i, (swap, dst) in enumerate(zip(swaps, (eg, eu, ed))):
        swap.wait_send()
        arrived(dst.at[1 - c], x_r.at[2 + i])
    home = g & 1
    arrived(psend.at[others], p_s.at[0])
    arrived(psend, p_s.at[1])
    for n in range(NCH):
        arrived(mbuf.at[n, above], m_r.at[n])
        sorted_rows = dot(onehot[...], wide_rows(mbuf[n])).astype(BF16)
        for k in range(PER):
            ysend[n, :, k] = sorted_rows[:, k * 128 : (k + 1) * 128].reshape(NG, 16, 128)

        def to_expert(k, n=n):
            return remote(
                ysend.at[n, k], ebuf.at[n, c, g >> 1], y_s, y_r.at[n], device(z, k, home)
            )

        for step in FAR_FIRST[NG][:-1]:
            to_expert(in_turn(g, NG, step)).start()

        @pl.when(home == c)
        def _(n=n):
            pltpu.make_async_copy(ysend.at[n, g], ebuf.at[n, c, g >> 1], y_r.at[n]).start()

        @pl.when(home != c)
        def _(to_expert=to_expert):
            to_expert(g).start()

    arrived(mbuf.at[:, above], m_s)

    gates, ups = [0.0, 0.0], [0.0, 0.0]
    for n in range(NCH):
        arrived(ebuf.at[n], y_r.at[n])
        for h in range(2):
            blocks = wide_rows(ebuf[n, h])
            rows_of = slice(h * half + n * PER * 128, h * half + (n + 1) * PER * 128)
            for f in range(2):
                gates[f] += dot(blocks, eg[f, rows_of])
                ups[f] += dot(blocks, eu[f, rows_of])
    hidden = jnp.concatenate(
        [(jax.nn.silu(gates[f]) * ups[f]).astype(BF16) for f in range(2)], axis=1
    )
    turns = [(dy, dd) for dy in (2, 1, 3, 0) for dd in (1, 0)]
    odd = (g ^ c) & 1
    for n in range(NCH):
        for h in range(2):
            cols_of = slice(h * half + n * PER * 128, h * half + (n + 1) * PER * 128)
            rows_out = dot(hidden, ed[:, :, cols_of].reshape(512, PER * 128)).astype(BF16)
            for j in range(PER):
                ret[n, h, :, j] = rows_out[:, j * 128 : (j + 1) * 128].reshape(8, 16, 128)
        for dy, dd in turns:
            k = ((g + 4 * dy) & 12) + ((g + odd + 2 * dd) & 3)
            for h in range(2):

                def give_back(k=k, n=n, h=h):
                    return remote(
                        ret.at[n, h, k >> 1], back.at[n, g], g_s, g_r.at[n], device(z, k, h)
                    )

                if (dy, dd) != (0, 0):
                    give_back().start()
                    continue
                here = jnp.logical_and(k == g, c == h)

                @pl.when(here)
                def _(n=n, h=h):
                    pltpu.make_async_copy(
                        ret.at[n, h, g >> 1], back.at[n, g], g_r.at[n]
                    ).start()

                @pl.when(jnp.logical_not(here))
                def _(give_back=give_back):
                    give_back().start()

    share.wait_recv()
    shared_out = (shs[pl.ds(c, 1)][0].astype(F32) + shb[...].astype(F32)).astype(BF16).astype(F32)
    arrived(ysend.at[:, others], y_s)

    @pl.when(home != c)
    def _():
        arrived(ysend.at[:, 0], y_s)

    share.wait_send()

    for n in range(NCH):
        arrived(back.at[n], g_r.at[n])
        answers = wide_rows(back[n])
        sums = (dot(comb_hi[...], answers) + dot(comb_lo[...], answers)).astype(BF16)
        for k in range(PER):
            csend[n, :, k] = sums[:, k * 128 : (k + 1) * 128].reshape(NZ, 16, 128)
        gh = column(lambda k, n=n: csend.at[n, k], lambda k, n=n: cbuf.at[n, k], h_s, h_r.at[n])
        gh.start()
        cbuf[n, pl.ds(z, 1)] = csend[n, pl.ds(z, 1)]
    arrived(back.at[:, others], g_s)

    @pl.when(home != c)
    def _():
        arrived(back.at[:, 0], g_s)

    for n in range(NCH):
        arrived(cbuf.at[n, above], h_r.at[n])
        part = slice(n * PER, (n + 1) * PER)
        mixs[part] = shared_out[part] + jnp.sum(cbuf[n].astype(F32), axis=0)
    last = remote(mixs, mixb, x_s.at[1], x_r.at[1], device(z, g, 1 - c))
    last.start()
    last.wait_recv()
    first_half = jnp.where(c == 0, mixs[...], mixb[...])
    second_half = jnp.where(c == 0, mixb[...], mixs[...])
    mixture = jnp.concatenate([first_half, second_half], axis=0)
    final = (middle[...].astype(F32) + mixture * row_scale(mixture) * outg_ref[...]).astype(BF16)
    for k in range(NG):
        result_ref[:, k * 128 : (k + 1) * 128] = final[k]
    arrived(csend.at[:, above], h_s)
    last.wait_send()
    store.wait()


def on_device(
    tokens, lengths, prior_state, mix_gain, post_gain, ffn_gain, out_gain,
    query_weight, key_weight, value_weight, gate_weight, out_weight, routes, route_gates,
    expert_gate, expert_up, expert_down, shared_gate, shared_up, shared_down,
):
    seq, width = tokens.shape
    frequency = THETA ** (-(np.arange(128) % 32).astype(np.float64) / 32)
    dma = pltpu.SemaphoreType.DMA
    blocks = pltpu.VMEM((NG, 16, 128), BF16)
    halves = pltpu.VMEM((NCH, NG, PER, 16, 128), BF16)
    columns_of = pltpu.VMEM((NCH, NZ, PER, 16, 128), BF16)
    vmem = pl.BlockSpec(memory_space=pltpu.VMEM)
    anywhere = pl.BlockSpec(memory_space=pl.ANY)
    big = (prior_state, expert_gate, expert_up, expert_down, shared_gate, shared_up, shared_down)
    chunk_sems = dma((NCH,))
    post, ffn, outer = (gain.reshape(NG, 1, 128) for gain in (post_gain, ffn_gain, out_gain))
    small = (
        tokens, routes.T, route_gates.T, lengths[None], jnp.asarray(frequency[None], F32),
        mix_gain[None], out_weight.T, post, ffn, outer,
    )
    columns = (query_weight, key_weight, value_weight, gate_weight)
    return pl.pallas_call(
        layer_kernel,
        out_shape=(
            pltpu.VMEM((seq, width), BF16),
            pltpu.VMEM(prior_state.shape, F32),
        ),
        in_specs=[anywhere] * (len(small) + len(columns) + len(big)),
        out_specs=(vmem, anywhere),
        scratch_shapes=[
            pltpu.VMEM(prior_state.shape, F32),
            *(pltpu.VMEM(array.shape, array.dtype) for array in small),
            *(pltpu.VMEM((2, *array.shape[1:]), BF16) for array in big[1:4]),
            *(pltpu.VMEM(array.shape, array.dtype) for array in big[4:]),
            blocks,
            pltpu.VMEM((16, 128), F32),
            pltpu.VMEM((16, 128), F32),
            pltpu.VMEM((2, 16, 128), F32),
            pltpu.VMEM((2, NG, seq, width // 2), BF16),
            blocks,
            pltpu.VMEM((NZ, NG, 16, 128), BF16),
            pltpu.VMEM((8, 16, 512), BF16),
            pltpu.VMEM((8, 16, 512), BF16),
            blocks,
            blocks,
            pltpu.VMEM((NZ, 16, 128), F32),
            pltpu.VMEM((16 * NG, 16 * NZ), BF16),
            pltpu.VMEM((16 * NZ, 16 * NG), BF16),
            pltpu.VMEM((16 * NZ, 16 * NG), BF16),
            pltpu.VMEM((4, 128, 16), F32),
            pltpu.VMEM((4, 128, 16), F32),
            pltpu.VMEM((8, 16, 128), F32),
            pltpu.VMEM((8, 16, 128), F32),
            pltpu.VMEM((8, 128), F32),
            pltpu.VMEM((2, NG, 2, 16, 128), BF16),
            blocks,
            pltpu.VMEM((2, NG, 16, 128), BF16),
            blocks,
            blocks,
            columns_of,
            pltpu.VMEM((2, 8, 16, 128), BF16),
            pltpu.VMEM((8, 16, 128), BF16),
            halves,
            pltpu.VMEM((NCH, 2, 8, PER, 16, 128), BF16),
            pltpu.VMEM((NCH, 2, 8, PER, 16, 128), BF16),
            halves,
            columns_of,
            columns_of,
            pltpu.VMEM((8, 16, 128), F32),
            pltpu.VMEM((8, 16, 128), F32),
            dma((len(small),)),
            dma,
            dma((8,)),
            dma, dma,
            dma, dma((NG,)),
            dma, dma,
            dma, dma, dma((NZ, 2)),
            dma, dma, dma, dma, dma, dma,
            dma, dma, dma, dma,
            dma((2,)), dma((2,)),
            dma, chunk_sems,
            dma, chunk_sems,
            dma, chunk_sems,
            dma, chunk_sems,
            dma((5,)), dma((5,)),
        ],
        compiler_params=pltpu.CompilerParams(
            collective_id=0, has_side_effects=True, vmem_limit_bytes=int(59.5 * 2**20)
        ),
        name="layer",
    )(
        *small,
        *columns,
        *big,
    )


def solution(mesh):
    finer = Mesh(mesh.devices.reshape(8, 4, 4, mesh.shape["tp"]), ("ep_0", "ep_1", "ep_2", "tp"))
    in_specs = (
        P(EP, None),
        P(EP),
        P(EP, "tp", None, None),
        P(),
        P(),
        P(),
        P(),
        P(EP, "tp"),
        P(EP, "tp"),
        P(EP, "tp"),
        P(EP, "tp"),
        P("tp", EP),
        P(EP, None),
        P(EP, None),
        P(EP, None, "tp"),
        P(EP, None, "tp"),
        P(EP, "tp", None),
        P(None, "tp"),
        P(None, "tp"),
        P("tp", None),
    )
    out_specs = (P(EP, None), P(EP, "tp", None, None))
    return jax.shard_map(
        on_device, mesh=finer, in_specs=in_specs, out_specs=out_specs, check_vma=False
    )
```

```python
import jax
import jax.numpy as jnp
import numpy as np
from jax import lax
from jax.experimental import pallas as pl
from jax.experimental.pallas import tpu as pltpu
from jax.sharding import Mesh
from jax.sharding import PartitionSpec as P

HEAD = 64
HEADS = 16
EP = ("ep_0", "ep_1", "ep_2")
EPS = 1e-06
THETA = 10000.0
MESH = pl.DeviceIdType.MESH
NZ, NY, NX, NG = 8, 4, 4, 16
NCH = 4
PER = 8 // NCH
FAR_FIRST = {
    NZ: sorted(range(NZ), key=lambda step: -min(step, NZ - step)),
    NG: sorted(
        range(NG), key=lambda step: (-min(step // 4, 4 - step // 4) - min(step % 4, 4 - step % 4), (step * 7) % 16)
    ),
}
BF16 = jnp.bfloat16
F32 = jnp.float32


def place():
    z, y, x, c = (lax.axis_index(name) for name in ("ep_0", "ep_1", "ep_2", "tp"))
    return z, y * NX + x, c


def device(z, g, c):
    return (z, g >> 2, g & 3, c)


def remote(src, dst, send_sem, recv_sem, target):
    return pltpu.make_async_remote_copy(
        src_ref=src,
        dst_ref=dst,
        send_sem=send_sem,
        recv_sem=recv_sem,
        device_id=target,
        device_id_type=MESH,
    )


def each(low, high, body):
    def step(i, carry):
        body(i)
        return carry

    lax.fori_loop(low, high, step, 0)


def dot(a, b, dims=((1,), (0,))):
    return lax.dot_general(a, b, (dims, ((), ())), preferred_element_type=F32)


def wide_rows(blocks):
    rows = blocks.shape[0] * blocks.shape[2]
    return jnp.concatenate(
        [blocks[:, k].reshape(rows, 128) for k in range(blocks.shape[1])], axis=1
    )


def row_scale(blocks):
    count = blocks.shape[0] * blocks.shape[2]
    total = jnp.sum(jnp.sum(blocks * blocks, axis=0), axis=-1, keepdims=True)
    return lax.rsqrt(total / count + EPS)[None]


def arrived(blocks, sem):
    pltpu.make_async_copy(blocks, blocks, sem).wait()


def in_turn(me, size, step):
    if size == NG:
        return ((me + 4 * (step // 4)) & 12) + ((me + step % 4) & 3)
    return (me + step) & (size - 1)


class Exchange:
    def __init__(self, me, size, at, src, dst, send, recv):
        self.me, self.size, self.at, self.src, self.dst = me, size, at, src, dst
        self.send, self.recv = send, recv

    def out(self, step):
        k = in_turn(self.me, self.size, step)
        return remote(self.src(k), self.dst(self.me), self.send, self.recv, self.at(k))

    def start(self, first=1):
        for step in FAR_FIRST[self.size]:
            if step >= first:
                self.out(step).start()


def layer_kernel(
    tokens_hbm, routes_hbm, gates_hbm, lengths_hbm, freq_hbm, mix_hbm, wot_hbm, post_hbm, ffn_hbm, outg_hbm,
    wq_hbm, wk_hbm, wv_hbm, wg_hbm,
    state_hbm, eg_hbm, eu_hbm, ed_hbm, sg_hbm, su_hbm, sd_hbm,
    result_ref, new_hbm,
    state,
    tokens_ref, routes_ref, gates_ref, lengths_ref, freq_ref, mix_ref, wot_ref, post_ref, ffn_ref, outg_ref,
    eg, eu, ed, sg, su, sd,
    wsrc, packed, rt, trig,
    tbuf, abuf, wbuf, zbuf, wo, osend, obuf, qbuf, onehot, comb_hi, comb_lo,
    qt, kt, vsc, fs, decays, rbuf, psend, pbuf, middle, mo, mbuf, shs, shb, ysend, ebuf, ret, back,
    csend, cbuf, mixs, mixb,
    i_s, v_s, w_s, a_s, a_r, t_s, t_r, u_s, u_r, b_s, n_s, b_r, c_s, c_r, d_s, d_r, q_s, q_r,
    o_s, o_r, r_s, r_r, p_s, p_r, m_s, m_r, y_s, y_r, g_s, g_r, h_s, h_r, x_s, x_r,
):
    z, g, c = place()
    loads = [
        pltpu.make_async_copy(src, dst, w_s.at[i])
        for i, (src, dst) in enumerate(
            ((state_hbm, state), (sg_hbm, sg), (su_hbm, su), (sd_hbm, sd),
             (eg_hbm.at[0], eg.at[c]), (eu_hbm.at[0], eu.at[c]), (ed_hbm.at[0], ed.at[c]))
        )
    ]
    barrier = pltpu.get_barrier_semaphore()

    def greet(target):
        pl.semaphore_signal(barrier, inc=1, device_id=target, device_id_type=MESH)

    for step in FAR_FIRST[NZ][:-1]:
        for core in range(2):
            greet(device((z + step) & (NZ - 1), g, core))
    for step in FAR_FIRST[NG]:
        k = in_turn(g, NG, step)
        if step:
            greet(device(z, k, c))
        greet(device(z, k, 1 - c))
    small = [
        pltpu.make_async_copy(src, dst, i_s.at[i])
        for i, (src, dst) in enumerate(
            ((tokens_hbm, tokens_ref), (mix_hbm, mix_ref), (routes_hbm, routes_ref),
             (gates_hbm, gates_ref), (lengths_hbm, lengths_ref), (freq_hbm, freq_ref),
             (wot_hbm, wot_ref), (post_hbm, post_ref), (ffn_hbm, ffn_ref), (outg_hbm, outg_ref))
        )
    ]
    slices = [
        pltpu.make_async_copy(
            w_ref.at[:, pl.ds(k * 128, 128)], wsrc.at[4 * m + k], v_s
        )
        for m, w_ref in enumerate((wq_hbm, wk_hbm, wv_hbm, wg_hbm))
        for k in range(4)
    ]
    for load in slices + small:
        load.start()
    arrived(wsrc, v_s)
    pl.semaphore_wait(barrier, 2 * NG - 1 + 2 * NZ - 2)

    def plane(src, dst, send, recv):
        return Exchange(g, NG, lambda k: device(z, k, c), src, dst, send, recv)

    def column(src, dst, send, recv):
        return Exchange(z, NZ, lambda k: device(k, g, c), src, dst, send, recv)

    others, above = pl.ds(0, NG - 1), pl.ds(0, NZ - 1)

    ga = plane(lambda k: wsrc.at[k], lambda k: abuf.at[k], a_s, a_r)
    gt = plane(lambda k: tbuf.at[c, g], lambda k: tbuf.at[c, k], t_s, t_r.at[g])
    gc = column(lambda k: wot_ref, lambda k: zbuf.at[k], c_s, c_r)
    gq = column(lambda k: rt, lambda k: qbuf.at[k], q_s, q_r)
    ga.start()
    pltpu.make_async_copy(wsrc.at[g], abuf.at[g], a_r).start()
    for load in small[:6]:
        load.wait()
    half = tbuf.shape[-1]
    wide = tokens_ref[...].astype(F32)
    scale = lax.rsqrt(jnp.mean(wide * wide, axis=-1, keepdims=True) + EPS)
    normed = (wide * scale * mix_ref[...]).astype(BF16)
    for k in range(2):
        tbuf[k, pl.ds(g, 1)] = normed[:, k * half : (k + 1) * half][None]
    packed[...] = jnp.zeros_like(packed)
    packed[0:6, 0:16] = routes_ref[...].astype(F32)
    packed[8:14, 0:16] = gates_ref[...]
    packed[14:15, 0:16] = lengths_ref[...].astype(F32)
    turned = packed[...].T[0:16]
    earlier = lax.broadcasted_iota(jnp.int32, (16, 16), 1) < lax.broadcasted_iota(
        jnp.int32, (16, 16), 0
    )
    column_of = lax.broadcasted_iota(jnp.int32, (16, 16), 1)
    table = turned
    for k in range(6):
        same = jnp.zeros((16, 16), F32)
        for other in range(6):
            same = jnp.where(
                turned[:, k : k + 1] == packed[other : other + 1, 0:16], 1.0, same
            )
        rank = jnp.max(jnp.where(earlier, same, 0.0), axis=1, keepdims=True)
        table = jnp.where(column_of == k, turned * 2.0 + rank, table)
    rt[:, 0:16] = table
    gq.start()
    for load in loads:
        load.start()
    qbuf[pl.ds(z, 1), :, 0:16] = rt[:, 0:16][None]

    arrived(abuf, a_r)

    def part_of(array, half_of):
        return array.at[pl.ds(half_of * 8, 8)]

    def b_copy(delta, half_of):
        return remote(
            part_of(abuf, half_of),
            part_of(wbuf.at[z], half_of),
            b_s,
            b_r.at[z, half_of],
            device((z + delta) & (NZ - 1), g, c),
        )

    for delta, half_of in ((2, 0), (-2, 0), (2, 1), (-2, 1), (1, 0), (-1, 0), (1, 1), (-1, 1)):
        b_copy(delta, half_of).start()
    for half_of in range(2):
        pltpu.make_async_copy(
            part_of(abuf, half_of), part_of(wbuf.at[z], half_of), b_r.at[z, half_of]
        ).start()
    gt.start()

    def b_wait(delta, half_of):
        source = (z + delta) & (NZ - 1)
        arrived(part_of(wbuf.at[source], half_of), b_r.at[source, half_of])

    def onward(delta, to, half_of):
        source = (z + delta) & (NZ - 1)
        block = part_of(wbuf.at[source], half_of)
        return remote(
            block, block, n_s, b_r.at[source, half_of], device((z + to) & (NZ - 1), g, c)
        )

    to_half = g >> 3

    def d_start(k):
        other = 2 * k + to_half

        @pl.when(other == g)
        def _():
            pltpu.make_async_copy(zbuf.at[k], wo.at[g & 7], d_r).start()

        @pl.when(other != g)
        def _():
            remote(zbuf.at[k], wo.at[g & 7], d_s, d_r, device(z, other, c)).start()

    for load in small[6:]:
        load.wait()
    arrived(qbuf.at[above], q_r)
    routing = qbuf[...].reshape(NZ * 16, 128)
    slots = 16 * NG
    row_z = lax.broadcasted_iota(jnp.int32, (NZ * 16, slots), 0) // 16
    lane = lax.broadcasted_iota(jnp.int32, (NZ * 16, slots), 1)
    slot_id = ((z * NG + lane // 16) * 2 + lane % 2).astype(F32)
    same_z = row_z == (lane % 16) // 2
    named = jnp.zeros((NZ * 16, slots), F32)
    weight = jnp.zeros((NZ * 16, slots), F32)
    for k in range(6):
        hit = jnp.logical_and(routing[:, k : k + 1] == slot_id, same_z)
        named = named + jnp.where(hit, 1.0, 0.0)
        weight = weight + jnp.where(hit, routing[:, 8 + k : 9 + k], 0.0)
    onehot[...] = named.T.astype(BF16)
    upper = weight.astype(BF16)
    comb_hi[...] = upper
    comb_lo[...] = (weight - upper.astype(F32)).astype(BF16)

    angles = rt[:, 14:15] * freq_ref[...]
    first = lax.broadcasted_iota(jnp.int32, (16, 128), 1) % 64 < 32
    trig[0] = jnp.cos(angles)
    sines = jnp.sin(angles)
    trig[1] = jnp.where(first, -sines, sines)
    heads = lax.broadcasted_iota(jnp.int32, (8, 128), 0) + c * 8
    decays[...] = 1.0 - jnp.exp2(-5.0 - 7.0 * heads.astype(F32) / (HEADS - 1))
    for half_of in range(2):
        b_wait(-2, half_of)
        onward(-2, 2, half_of).start()
        onward(-2, 1, half_of).start()
        b_wait(2, half_of)
        onward(2, -1, half_of).start()

    def t_forward(half_of, k):
        block = tbuf.at[half_of, k]
        return remote(block, block, u_s, u_r, device(z, g, 1 - c))

    for step in FAR_FIRST[NG][:-1]:
        k = in_turn(g, NG, step)
        arrived(tbuf.at[c, k], t_r.at[k])
        t_forward(c, k).start()
    arrived(tbuf.at[1 - c, others], u_r)

    for delta in (0, 1, -1, 3, -3, 4):
        b_wait(delta, 0)
        b_wait(delta, 1)
    rows = NG * tbuf.shape[2]
    mine = dot(tbuf[0].reshape(rows, half), wbuf[0:4].reshape(half, 128)) + dot(
        tbuf[1].reshape(rows, half), wbuf[4:8].reshape(half, 128)
    )
    osend[...] = mine.astype(BF16).reshape(osend.shape)
    go = plane(lambda k: osend.at[k], lambda k: obuf.at[k], o_s, o_r)
    go.start()
    gc = column(lambda k: wot_ref, lambda k: zbuf.at[z], c_s, c_r)
    gc.start()
    pltpu.make_async_copy(wot_ref, zbuf.at[z], c_r).start()
    obuf[pl.ds(g, 1)] = osend[pl.ds(g, 1)]
    arrived(abuf.at[others], a_s)
    arrived(tbuf.at[c, others], t_s)
    arrived(tbuf.at[c, others], u_s)
    arrived(qbuf.at[above], q_s)
    arrived(wbuf.at[pl.ds(0, 4)], b_s)
    arrived(wbuf.at[pl.ds(0, 3)], n_s)
    loads[0].wait()
    arrived(obuf.at[others], o_r)
    arrived(zbuf, c_r)
    each(0, NZ, d_start)
    swaps = [
        remote(src.at[0], dst.at[c], x_s.at[2 + i], x_r.at[2 + i], device(z, g, 1 - c))
        for i, (src, dst) in enumerate(((eg_hbm, eg), (eu_hbm, eu), (ed_hbm, ed)))
    ]
    for swap in swaps:
        swap.start()
    low_half = lax.broadcasted_iota(jnp.int32, (16, 128), 1) < 64
    def rotate(v):
        other = jnp.where(first, pltpu.roll(v, 96, 1), pltpu.roll(v, 32, 1))
        return v * trig[0] + other * trig[1]

    def by_head(v):
        low = jnp.sum(jnp.where(low_half, v, 0.0), axis=-1, keepdims=True)
        high = jnp.sum(jnp.where(low_half, 0.0, v), axis=-1, keepdims=True)
        return jnp.where(low_half, low, high)

    def block(k, hp):
        return obuf[4 * k + hp].astype(F32)

    self_terms = []
    for hp in range(4):
        query = rotate(block(0, hp))
        key = rotate(block(1, hp)) * HEAD ** (-0.5)
        value = block(2, hp)
        qt[hp] = query.T
        kt[hp] = key.T
        vsc[2 * hp] = value
        vsc[2 * hp + 1] = pltpu.roll(value, 64, 1)
        self_terms.append(by_head(query * key) * value)

    def read_pair(hp):
        queries = qt[pl.ds(hp, 1)][0]
        for h in range(2):
            for s in range(16):
                held = state[s, pl.ds(2 * hp + h, 1)][0]
                column_q = queries[h * 64 : (h + 1) * 64, s : s + 1]
                fs[pl.ds(2 * hp + h, 1), s : s + 1, 0:64] = jnp.sum(
                    column_q * held, axis=0, keepdims=True
                )[None]

    for part in range(2):
        each(2 * part, 2 * part + 2, read_pair)
        for hp in (2 * part, 2 * part + 1):
            from_state = jnp.where(low_half, fs[2 * hp], pltpu.roll(fs[2 * hp + 1], 64, 1))
            decay = jnp.where(
                low_half[0:1], decays[2 * hp : 2 * hp + 1], decays[2 * hp + 1 : 2 * hp + 2]
            )
            read = decay * from_state + self_terms[hp]
            read = read * lax.rsqrt(by_head(read * read) / HEAD + EPS)
            rbuf[part, pl.ds(g, 1), hp & 1] = (read * jax.nn.silu(block(3, hp))).astype(BF16)[None]
        plane(
            lambda k, part=part: rbuf.at[part, g], lambda k, part=part: rbuf.at[part, g], r_s, r_r
        ).start()

    def update_pair(hp):
        keys = kt[pl.ds(hp, 1)][0]
        for h in range(2):
            decay = decays[pl.ds(2 * hp + h, 1), 0:64]
            value = vsc[pl.ds(2 * hp + h, 1)][0]
            for s in range(16):
                held = state[s, pl.ds(2 * hp + h, 1)][0]
                column_k = keys[h * 64 : (h + 1) * 64, s : s + 1]
                state[s, pl.ds(2 * hp + h, 1)] = (
                    decay * held + column_k * value[s : s + 1, 0:64]
                )[None]

    each(0, 4, update_pair)
    def d_wait(k):
        pltpu.make_async_copy(zbuf.at[k], wo.at[k], d_r.at[k]).wait()

    store = pltpu.make_async_copy(state, new_hbm, w_s.at[7])
    store.start()
    arrived(obuf.at[others], o_s)
    arrived(zbuf.at[above], c_s)

    @pl.when((g & 1) == to_half)
    def _():
        arrived(zbuf.at[above], d_s)

    @pl.when((g & 1) != to_half)
    def _():
        arrived(zbuf, d_s)

    arrived(wo, d_r)
    arrived(rbuf.at[:, others], r_r)
    partial = dot(
        jnp.concatenate([wide_rows(rbuf[0]), wide_rows(rbuf[1])], axis=1),
        wo[...].reshape(128, 512),
        ((1,), (1,)),
    )
    psend[...] = partial.astype(BF16).reshape(psend.shape)
    gp = plane(lambda k: psend.at[k], lambda k: pbuf.at[c, k], p_s.at[0], p_r.at[0])
    gp_other = Exchange(
        g, NG, lambda k: device(z, k, 1 - c), lambda k: psend.at[k], lambda k: pbuf.at[c, k],
        p_s.at[1], p_r.at[1],
    )
    for step in FAR_FIRST[NG]:
        if step:
            gp.out(step).start()
        gp_other.out(step).start()
    pbuf[pl.ds(c, 1), pl.ds(g, 1)] = psend[pl.ds(g, 1)][None]
    arrived(rbuf.at[:, others], r_s)
    arrived(psend.at[others], p_r.at[0])
    arrived(psend, p_r.at[1])
    mixed = (pbuf[0].astype(F32) + pbuf[1].astype(F32)).astype(BF16).astype(F32)
    tok = jnp.stack([tokens_ref[:, k * 128 : (k + 1) * 128] for k in range(NG)]).astype(F32)
    mid = (tok + mixed * row_scale(mixed) * post_ref[...]).astype(BF16)
    middle[...] = mid
    mid = mid.astype(F32)
    mo[...] = (mid * row_scale(mid) * ffn_ref[...]).astype(BF16)

    for n in range(NCH):
        blocks = pl.ds(c * 8 + n * PER, PER)
        mbuf[n, pl.ds(z, 1)] = mo[blocks][None]
        gm = column(lambda k, n=n: mbuf.at[n, z], lambda k, n=n: mbuf.at[n, k], m_s, m_r.at[n])
        gm.start()
    for load in loads[1:4]:
        load.wait()
    rows_in = wide_rows(mo[...][None])
    shared_hidden = (jax.nn.silu(dot(rows_in, sg[...])) * dot(rows_in, su[...])).astype(BF16)
    shared_part = dot(shared_hidden, sd[...]).astype(BF16)
    parts = jnp.stack([shared_part[:, k * 128 : (k + 1) * 128] for k in range(NG)])
    shs[...] = parts.reshape(shs.shape)
    share = remote(shs.at[1 - c], shb, x_s.at[0], x_r.at[0], device(z, g, 1 - c))
    share.start()
    for load in loads[4:]:
        load.wait()
    for i, (swap, dst) in enumerate(zip(swaps, (eg, eu, ed))):
        swap.wait_send()
        arrived(dst.at[1 - c], x_r.at[2 + i])
    home = g & 1
    arrived(psend.at[others], p_s.at[0])
    arrived(psend, p_s.at[1])
    for n in range(NCH):
        arrived(mbuf.at[n, above], m_r.at[n])
        sorted_rows = dot(onehot[...], wide_rows(mbuf[n])).astype(BF16)
        for k in range(PER):
            ysend[n, :, k] = sorted_rows[:, k * 128 : (k + 1) * 128].reshape(NG, 16, 128)

        def to_expert(k, n=n):
            return remote(
                ysend.at[n, k], ebuf.at[n, c, g >> 1], y_s, y_r.at[n], device(z, k, home)
            )

        for step in FAR_FIRST[NG][:-1]:
            to_expert(in_turn(g, NG, step)).start()

        @pl.when(home == c)
        def _(n=n):
            pltpu.make_async_copy(ysend.at[n, g], ebuf.at[n, c, g >> 1], y_r.at[n]).start()

        @pl.when(home != c)
        def _(to_expert=to_expert):
            to_expert(g).start()

    arrived(mbuf.at[:, above], m_s)

    gates, ups = [0.0, 0.0], [0.0, 0.0]
    for n in range(NCH):
        arrived(ebuf.at[n], y_r.at[n])
        for h in range(2):
            blocks = wide_rows(ebuf[n, h])
            rows_of = slice(h * half + n * PER * 128, h * half + (n + 1) * PER * 128)
            for f in range(2):
                gates[f] += dot(blocks, eg[f, rows_of])
                ups[f] += dot(blocks, eu[f, rows_of])
    hidden = jnp.concatenate(
        [(jax.nn.silu(gates[f]) * ups[f]).astype(BF16) for f in range(2)], axis=1
    )
    turns = [(dy, dd) for dy in (2, 1, 3, 0) for dd in (1, 0)]
    odd = (g ^ c) & 1
    for n in range(NCH):
        for h in range(2):
            cols_of = slice(h * half + n * PER * 128, h * half + (n + 1) * PER * 128)
            rows_out = dot(hidden, ed[:, :, cols_of].reshape(512, PER * 128)).astype(BF16)
            for j in range(PER):
                ret[n, h, :, j] = rows_out[:, j * 128 : (j + 1) * 128].reshape(8, 16, 128)
        for dy, dd in turns:
            k = ((g + 4 * dy) & 12) + ((g + odd + 2 * dd) & 3)
            for h in range(2):

                def give_back(k=k, n=n, h=h):
                    return remote(
                        ret.at[n, h, k >> 1], back.at[n, g], g_s, g_r.at[n], device(z, k, h)
                    )

                if (dy, dd) != (0, 0):
                    give_back().start()
                    continue
                here = jnp.logical_and(k == g, c == h)

                @pl.when(here)
                def _(n=n, h=h):
                    pltpu.make_async_copy(
                        ret.at[n, h, g >> 1], back.at[n, g], g_r.at[n]
                    ).start()

                @pl.when(jnp.logical_not(here))
                def _(give_back=give_back):
                    give_back().start()

    share.wait_recv()
    shared_out = (shs[pl.ds(c, 1)][0].astype(F32) + shb[...].astype(F32)).astype(BF16).astype(F32)
    arrived(ysend.at[:, others], y_s)

    @pl.when(home != c)
    def _():
        arrived(ysend.at[:, 0], y_s)

    share.wait_send()

    for n in range(NCH):
        arrived(back.at[n], g_r.at[n])
        answers = wide_rows(back[n])
        sums = (dot(comb_hi[...], answers) + dot(comb_lo[...], answers)).astype(BF16)
        for k in range(PER):
            csend[n, :, k] = sums[:, k * 128 : (k + 1) * 128].reshape(NZ, 16, 128)
        gh = column(lambda k, n=n: csend.at[n, k], lambda k, n=n: cbuf.at[n, k], h_s, h_r.at[n])
        gh.start()
        cbuf[n, pl.ds(z, 1)] = csend[n, pl.ds(z, 1)]
    arrived(back.at[:, others], g_s)

    @pl.when(home != c)
    def _():
        arrived(back.at[:, 0], g_s)

    for n in range(NCH):
        arrived(cbuf.at[n, above], h_r.at[n])
        part = slice(n * PER, (n + 1) * PER)
        mixs[part] = shared_out[part] + jnp.sum(cbuf[n].astype(F32), axis=0)
    last = remote(mixs, mixb, x_s.at[1], x_r.at[1], device(z, g, 1 - c))
    last.start()
    last.wait_recv()
    first_half = jnp.where(c == 0, mixs[...], mixb[...])
    second_half = jnp.where(c == 0, mixb[...], mixs[...])
    mixture = jnp.concatenate([first_half, second_half], axis=0)
    final = (middle[...].astype(F32) + mixture * row_scale(mixture) * outg_ref[...]).astype(BF16)
    for k in range(NG):
        result_ref[:, k * 128 : (k + 1) * 128] = final[k]
    arrived(csend.at[:, above], h_s)
    last.wait_send()
    store.wait()


def on_device(
    tokens, lengths, prior_state, mix_gain, post_gain, ffn_gain, out_gain,
    query_weight, key_weight, value_weight, gate_weight, out_weight, routes, route_gates,
    expert_gate, expert_up, expert_down, shared_gate, shared_up, shared_down,
):
    seq, width = tokens.shape
    frequency = THETA ** (-(np.arange(128) % 32).astype(np.float64) / 32)
    dma = pltpu.SemaphoreType.DMA
    blocks = pltpu.VMEM((NG, 16, 128), BF16)
    halves = pltpu.VMEM((NCH, NG, PER, 16, 128), BF16)
    columns_of = pltpu.VMEM((NCH, NZ, PER, 16, 128), BF16)
    vmem = pl.BlockSpec(memory_space=pltpu.VMEM)
    anywhere = pl.BlockSpec(memory_space=pl.ANY)
    big = (prior_state, expert_gate, expert_up, expert_down, shared_gate, shared_up, shared_down)
    chunk_sems = dma((NCH,))
    post, ffn, outer = (gain.reshape(NG, 1, 128) for gain in (post_gain, ffn_gain, out_gain))
    small = (
        tokens, routes.T, route_gates.T, lengths[None], jnp.asarray(frequency[None], F32),
        mix_gain[None], out_weight.T, post, ffn, outer,
    )
    columns = (query_weight, key_weight, value_weight, gate_weight)
    return pl.pallas_call(
        layer_kernel,
        out_shape=(
            pltpu.VMEM((seq, width), BF16),
            pltpu.VMEM(prior_state.shape, F32),
        ),
        in_specs=[anywhere] * (len(small) + len(columns) + len(big)),
        out_specs=(vmem, anywhere),
        scratch_shapes=[
            pltpu.VMEM(prior_state.shape, F32),
            *(pltpu.VMEM(array.shape, array.dtype) for array in small),
            *(pltpu.VMEM((2, *array.shape[1:]), BF16) for array in big[1:4]),
            *(pltpu.VMEM(array.shape, array.dtype) for array in big[4:]),
            blocks,
            pltpu.VMEM((16, 128), F32),
            pltpu.VMEM((16, 128), F32),
            pltpu.VMEM((2, 16, 128), F32),
            pltpu.VMEM((2, NG, seq, width // 2), BF16),
            blocks,
            pltpu.VMEM((NZ, NG, 16, 128), BF16),
            pltpu.VMEM((8, 16, 512), BF16),
            pltpu.VMEM((8, 16, 512), BF16),
            blocks,
            blocks,
            pltpu.VMEM((NZ, 16, 128), F32),
            pltpu.VMEM((16 * NG, 16 * NZ), BF16),
            pltpu.VMEM((16 * NZ, 16 * NG), BF16),
            pltpu.VMEM((16 * NZ, 16 * NG), BF16),
            pltpu.VMEM((4, 128, 16), F32),
            pltpu.VMEM((4, 128, 16), F32),
            pltpu.VMEM((8, 16, 128), F32),
            pltpu.VMEM((8, 16, 128), F32),
            pltpu.VMEM((8, 128), F32),
            pltpu.VMEM((2, NG, 2, 16, 128), BF16),
            blocks,
            pltpu.VMEM((2, NG, 16, 128), BF16),
            blocks,
            blocks,
            columns_of,
            pltpu.VMEM((2, 8, 16, 128), BF16),
            pltpu.VMEM((8, 16, 128), BF16),
            halves,
            pltpu.VMEM((NCH, 2, 8, PER, 16, 128), BF16),
            pltpu.VMEM((NCH, 2, 8, PER, 16, 128), BF16),
            halves,
            columns_of,
            columns_of,
            pltpu.VMEM((8, 16, 128), F32),
            pltpu.VMEM((8, 16, 128), F32),
            dma((len(small),)),
            dma,
            dma((8,)),
            dma, dma,
            dma, dma((NG,)),
            dma, dma,
            dma, dma, dma((NZ, 2)),
            dma, dma, dma, dma, dma, dma,
            dma, dma, dma, dma,
            dma((2,)), dma((2,)),
            dma, chunk_sems,
            dma, chunk_sems,
            dma, chunk_sems,
            dma, chunk_sems,
            dma((5,)), dma((5,)),
        ],
        compiler_params=pltpu.CompilerParams(
            collective_id=0, has_side_effects=True, vmem_limit_bytes=int(59.5 * 2**20)
        ),
        name="layer",
    )(
        *small,
        *columns,
        *big,
    )


def solution(mesh):
    finer = Mesh(mesh.devices.reshape(8, 4, 4, mesh.shape["tp"]), ("ep_0", "ep_1", "ep_2", "tp"))
    in_specs = (
        P(EP, None),
        P(EP),
        P(EP, "tp", None, None),
        P(),
        P(),
        P(),
        P(),
        P(EP, "tp"),
        P(EP, "tp"),
        P(EP, "tp"),
        P(EP, "tp"),
        P("tp", EP),
        P(EP, None),
        P(EP, None),
        P(EP, None, "tp"),
        P(EP, None, "tp"),
        P(EP, "tp", None),
        P(None, "tp"),
        P(None, "tp"),
        P("tp", None),
    )
    out_specs = (P(EP, None), P(EP, "tp", None, None))
    return jax.shard_map(
        on_device, mesh=finer, in_specs=in_specs, out_specs=out_specs, check_vma=False
    )
```
